32 devices in a mesh: sp: 16 (over z, y, x), tp: 2 (over core).
Axes of the slice: x: 2, y: 2, z: 4, core: 2. Of those that a mesh axis runs over, the one named last changes fastest.
Arguments:
- tokens: bfloat16 [4096, 2048], P('sp', 'tp'), may hold values from -6 to 6
- outer_gate: bfloat16 [2048, 1024], P(None, 'tp'), may hold values from -0.125 to 0.125
- inner_gate: bfloat16 [2048, 1024], P(None, 'tp'), may hold values from -0.125 to 0.125
- conv_input: bfloat16 [2048, 1024], P(None, 'tp'), may hold values from -0.125 to 0.125
- conv_taps: bfloat16 [3, 1024], P(None, 'tp'), may hold values from -3.5 to 3.5
- query_down: bfloat16 [2048, 512], P(None, 'tp'), may hold values from -0.125 to 0.125
- latent_down: bfloat16 [2048, 256], P(None, 'tp'), may hold values from -0.125 to 0.125
- rotary_down: bfloat16 [2048, 32], replicated, may hold values from -5.303301 to 5.303301
- query_gain: float32 [512], replicated, may hold values from 0.1 to 1.9
- latent_gain: float32 [256], replicated, may hold values from 0.1 to 1.9
- query_up: bfloat16 [512, 1536], P(None, 'tp'), may hold values from -0.52734375 to 0.52734375
- latent_up: bfloat16 [256, 2048], P(None, 'tp'), may hold values from -0.75 to 0.75
- conv_project: bfloat16 [1024, 2048], P('tp'), may hold values from -0.1875 to 0.1875
- attend_project: bfloat16 [1024, 2048], P('tp'), may hold values from -0.1875 to 0.1875
Outputs:
- mixed: bfloat16 [4096, 2048], P(('sp', 'tp'))
The draws below stay inside these ranges and needn't reach their ends.
All inputs are finite; a program needn't handle non-finite values.
Results may differ from the reference program's by a relative error of at most 0.035.
Values may be sent and summed in bfloat16 or wider, within the bound.
A program may use at most 128 MiB of HBM per device.

```python
import math
import jax
import jax.numpy as jnp
from jax import lax

D = 2048
CW = 1024
HEADS = 16
QR = 512
KVR = 256
NOPE = 64
ROPE = 32
VDIM = 64
KSIZE = 3
TOKENS = 4096
N_TP = 2


def draw_rotary_down(key, part):
    base = jnp.clip(jax.random.normal(key, (D, ROPE), jnp.float32), -6.0, 6.0) * D ** (-0.5)
    return base.astype(jnp.bfloat16)


def steps_of(own_key, dims, shards, smallest, high):
    def one(dim, parts):
        draws = jax.random.uniform(jax.random.fold_in(jax.random.fold_in(own_key, 6), dim), (parts,), jnp.float32, smallest / len(shards), high / len(shards))
        return jnp.repeat(jnp.exp(draws), dims[dim] // parts).reshape((-1,) + (1,) * (len(dims) - dim - 1))

    loudness = one(*shards[0])
    for cut in shards[1:]:
        loudness = loudness * one(*cut)
    return loudness


def noise(stream_key, dims, deviation, most, shards=(), held_as=jnp.bfloat16):
    values = deviation * jax.random.normal(stream_key, dims, jnp.float32)
    if shards:
        values = values * steps_of(stream_key, dims, shards, -0.22, 0.18)
    return jnp.clip(values, -most, most).astype(held_as)


def setup_inputs(seed: int = 0) -> dict:
    keys = jax.random.split(jax.random.key(seed), 15)
    tokens = noise(keys[0], (TOKENS, D), 1.0, 6.0, ((0, 16), (1, 2)))
    outer_gate = noise(keys[1], (D, CW), D ** -0.5, 0.125, ((1, 2),))
    inner_gate = noise(keys[2], (D, CW), D ** -0.5, 0.125, ((1, 2),))
    conv_input = noise(keys[3], (D, CW), D ** -0.5, 0.125, ((1, 2),))
    conv_taps = noise(keys[4], (KSIZE, CW), KSIZE ** -0.5, 3.5, ((1, 2),))
    query_down = noise(keys[5], (D, QR), D ** -0.5, 0.125, ((1, 2),))
    latent_down = noise(keys[6], (D, KVR), D ** -0.5, 0.125, ((1, 2),))
    rotary_down = draw_rotary_down(jax.random.fold_in(keys[14], 71), 0)
    query_gain = jnp.clip(1.0 + 0.18 * jax.random.normal(keys[8], (QR,), jnp.float32), 0.1, 1.9)
    latent_gain = jnp.clip(1.0 + 0.18 * jax.random.normal(keys[9], (KVR,), jnp.float32), 0.1, 1.9)
    query_up = noise(keys[10], (QR, HEADS * (NOPE + ROPE)), (2.0 / QR ** 0.5), 0.52734375, ((1, 2),))
    latent_up = noise(keys[11], (KVR, HEADS * (NOPE + VDIM)), (2.0 / KVR ** 0.5), 0.75, ((1, 2),))
    conv_project = noise(keys[12], (CW, D), CW ** -0.5, 0.1875, ((0, 2),))
    attend_project = noise(keys[13], (HEADS * VDIM, D), (HEADS * VDIM) ** -0.5, 0.1875, ((0, 2),))
    return {"tokens": tokens, "outer_gate": outer_gate, "inner_gate": inner_gate, "conv_input": conv_input, "conv_taps": conv_taps, "query_down": query_down, "latent_down": latent_down, "rotary_down": rotary_down, "query_gain": query_gain, "latent_gain": latent_gain, "query_up": query_up, "latent_up": latent_up, "conv_project": conv_project, "attend_project": attend_project}


neg_fill = -1e+30
rotary_base = 10000.0
norm_epsilon = 1e-06

def matmul(left, right):
    return jnp.dot(left, right, preferred_element_type=jnp.float32)

def rotate(values, positions):
    half = values.shape[-1] // 2
    inverse = rotary_base ** (-(jnp.arange(half, dtype=jnp.float32) * 2.0 / (2 * half)))
    angle = positions[:, None] * inverse[None, :]
    if values.ndim == 3:
        angle = angle[:, None, :]
    cosine = jnp.cos(angle)
    sine = jnp.sin(angle)
    first = values[..., :half]
    second = values[..., half:]
    return jnp.concatenate([first * cosine - second * sine, first * sine + second * cosine], -1)

def rms_scale(latent, gain):
    values = lax.optimization_barrier(latent).astype(jnp.float32)
    factor = lax.rsqrt(lax.optimization_barrier(jnp.mean(values * values, -1, keepdims=True)) + norm_epsilon)
    return (values * factor * gain).astype(jnp.bfloat16)

def reference(tokens, outer_gate, inner_gate, conv_input, conv_taps, query_down, latent_down, rotary_down, query_gain, latent_gain, query_up, latent_up, conv_project, attend_project):
    length = tokens.shape[0]
    outer = matmul(tokens, outer_gate)
    inner = matmul(tokens, inner_gate)
    signal = matmul(tokens, conv_input)
    gated = lax.optimization_barrier((inner * signal).astype(jnp.bfloat16)).astype(jnp.float32)
    padded = jnp.pad(gated, ((KSIZE - 1, 0), (0, 0)))
    taps = conv_taps.astype(jnp.float32)
    filtered = padded[0:length] * taps[0]
    for index in range(1, KSIZE):
        filtered = filtered + padded[index:index + length] * taps[index]
    conv_result = (outer * filtered).astype(jnp.bfloat16)
    positions = jnp.arange(length, dtype=jnp.float32)
    query_norm = rms_scale(matmul(tokens, query_down).astype(jnp.bfloat16), query_gain)
    latent_norm = rms_scale(matmul(tokens, latent_down).astype(jnp.bfloat16), latent_gain)
    rotary_key = rotate(matmul(tokens, rotary_down), positions).astype(jnp.bfloat16)
    query_full = matmul(query_norm, query_up).reshape(length, HEADS, NOPE + ROPE)
    query_plain = query_full[..., :NOPE].astype(jnp.bfloat16).astype(jnp.float32)
    query_rot = rotate(query_full[..., NOPE:], positions).astype(jnp.bfloat16).astype(jnp.float32)
    expanded = matmul(latent_norm, latent_up).astype(jnp.bfloat16).reshape(length, HEADS, NOPE + VDIM)
    key_plain = expanded[..., :NOPE].astype(jnp.float32)
    values = expanded[..., NOPE:].astype(jnp.float32)
    key_rot = rotary_key.astype(jnp.float32)
    scale = (NOPE + ROPE) ** (-0.5)
    block = math.gcd(length, 256)
    key_index = jnp.arange(length)

    def one_block(number):
        first = (number * block).astype(jnp.int32)
        plain = lax.dynamic_slice_in_dim(query_plain, first, block, 0)
        turned = lax.dynamic_slice_in_dim(query_rot, first, block, 0)
        scores = jnp.einsum('qhd,khd->hqk', plain, key_plain) + jnp.einsum('qhr,kr->hqk', turned, key_rot)
        scores = scores * scale
        query_index = first + jnp.arange(block)
        visible = key_index[None, :] <= query_index[:, None]
        scores = jnp.where(visible[None], scores, neg_fill)
        rowmax = lax.optimization_barrier(jnp.max(scores, -1, keepdims=True))
        weight = jnp.exp(scores - rowmax)
        total = lax.optimization_barrier(jnp.sum(weight, -1))
        rounded = weight.astype(jnp.bfloat16).astype(jnp.float32)
        summed = jnp.einsum('hqk,khd->qhd', rounded, values)
        return (summed / total.T[:, :, None]).astype(jnp.bfloat16)
    attended = lax.map(one_block, jnp.arange(length // block, dtype=jnp.int32))
    attended = attended.reshape(length, HEADS * VDIM)
    conv_share = CW // N_TP
    head_share = HEADS * VDIM // N_TP
    result = jnp.zeros((length, D), jnp.float32)
    for group in range(N_TP):
        partial_value = matmul(conv_result[:, group * conv_share:(group + 1) * conv_share], conv_project[group * conv_share:(group + 1) * conv_share])
        partial_value = partial_value + matmul(attended[:, group * head_share:(group + 1) * head_share], attend_project[group * head_share:(group + 1) * head_share])
        result = result + lax.optimization_barrier(partial_value.astype(jnp.bfloat16)).astype(jnp.float32)
    return result.astype(jnp.bfloat16)
```

```python
import jax
import numpy as np
import jax.numpy as jnp
from jax import lax
from jax.experimental import pallas as pl
from jax.experimental.pallas import tpu as pltpu
from jax.sharding import PartitionSpec as P

NOPE = 64
ROPE = 32
VDIM = 64
LANES = 128
ONES = 16
EDGE = 16
RING = 8
LAG = 2

MESH = pl.DeviceIdType.MESH
neg_fill = -1e30
rotary_base = 10000.0
norm_epsilon = 1e-06
log2e = 1.4426950408889634


def dot(a, b, dims=((1,), (0,))):
    return lax.dot_general(a, b, (dims, ((), ())), preferred_element_type=jnp.float32)


def unit(lat_parts, rot_parts, qx_ref, wk_ref, wvt_ref, keys, turned, scores, weights, best_ref, acc_ref, masked):
    heads, _, rows = qx_ref.shape
    latent = jnp.concatenate(lat_parts, 0)
    rot = jnp.concatenate(rot_parts, 0)
    span = latent.shape[0]
    keys[:span] = dot(latent, wk_ref[...]).astype(jnp.bfloat16)
    flat = dot(wvt_ref[...], latent, ((1,), (1,))).astype(jnp.bfloat16)
    for h in range(heads):
        turned[h, :VDIM, :span] = flat[h * VDIM : (h + 1) * VDIM]
    ring = scores.shape[0]
    tops = [None] * heads

    def score(h):
        pair = h // 2 * 2 * NOPE
        key = jnp.concatenate([keys[:span, pair : pair + 2 * NOPE], rot], 1)
        s = dot(key, qx_ref[h])
        if masked:
            k_at = lax.broadcasted_iota(jnp.int32, s.shape, 0)
            q_at = lax.broadcasted_iota(jnp.int32, s.shape, 1)
            s = jnp.where(k_at <= q_at, s, neg_fill)
        scores[h % ring, :span] = s
        top = jnp.max(s, 0, keepdims=True)
        if masked:
            tops[h] = (top, None)
        else:
            old = best_ref[h]
            top = jnp.maximum(old, top)
            tops[h] = (top, jnp.exp2(old - top))
        best_ref[h] = top

    def soften(h):
        weights[h % ring, :span] = jnp.exp2((scores[h % ring, :span] - tops[h][0]).astype(jnp.bfloat16))

    def gather(h):
        fresh = dot(turned[h, :, :span], weights[h % ring, :span])
        acc_ref[h] = fresh if masked else acc_ref[h] * tops[h][1] + fresh

    for step in range(heads + 2 * LAG):
        if step < heads:
            score(step)
        if 0 <= step - LAG < heads:
            soften(step - LAG)
        if 0 <= step - 2 * LAG < heads:
            gather(step - 2 * LAG)


def mix_kernel(
    tok_in, inv_ref, taps_ref, qgain_ref, lgain_ref,
    ldown_in, qdown_in, rdown_in, inner_in, signal_in, up_in, qup_in, outer_in, cproj_in, aproj_in,
    out_ref,
    tok, ldown, qdown, rdown, inner_w, signal_w, up_ref, qup, outer_w, cproj_ref, aproj_ref,
    xbuf, raw_lat, raw_query, edge, rim, padded, conv_ref, wk_ref, wvt_ref, qx_ref,
    kv, keys, turned, scores, weights, best_ref, acc_ref, att, early, cpart, part_buf, in_buf,
    load_sem, front_send, front_recv, up_send, side_send, kv_recv, share_send, share_recv, tail_send, tail_recv,
):
    me = lax.axis_index("sp")
    t = lax.axis_index("tp")
    total = lax.axis_size("sp")
    ways = lax.axis_size("tp")
    planes = total // 4
    z = me // 4
    b0 = me % 2
    b1 = (me // 2) % 2
    heads, _, rows = qx_ref.shape
    short = rows // ways
    cross = (1 - 2 * b0, 2 - 4 * b1, 3 - 2 * b0 - 4 * b1)
    after = lax.rem(me + 1, total)
    before = lax.rem(me + total - 1, total)
    mates = [lax.rem(t + o, ways) for o in range(1, ways)]

    barrier = pltpu.get_barrier_semaphore()
    targets = [(me, mate) for mate in mates] + [(me + c, t) for c in cross]
    targets += [(lax.rem(me + 4 * d, total), t) for d in range(1, planes)] + [(after, t), (before, t)]
    for target in targets:
        pl.semaphore_signal(barrier, inc=1, device_id=target, device_id_type=MESH)

    pairs = (
        (tok_in, tok), (ldown_in, ldown), (qdown_in, qdown), (rdown_in, rdown), (inner_in, inner_w), (signal_in, signal_w),
        (up_in, up_ref), (qup_in, qup), (outer_in, outer_w), (cproj_in, cproj_ref), (aproj_in, aproj_ref),
    )
    loads = [pltpu.make_async_copy(a, b, load_sem.at[i]) for i, (a, b) in enumerate(pairs)]
    for copy in loads:
        copy.start()

    position = (me * rows + lax.broadcasted_iota(jnp.int32, (1, rows), 1)).astype(jnp.float32)
    angle = inv_ref[...] * position
    cosine = jnp.cos(angle)
    sine = jnp.sin(angle)
    half = ROPE // 2

    def rotated(values):
        a = values[:half]
        b = values[half:]
        return jnp.concatenate([a * cosine - b * sine, a * sine + b * cosine], 0).astype(jnp.bfloat16)

    for h in range(heads):
        turned[h, VDIM:] = jnp.ones((ONES, turned.shape[2]), jnp.bfloat16)
    pl.semaphore_wait(barrier, len(targets))
    loads[0].wait()

    def to_mates(source, slots, kind):
        return [
            pltpu.make_async_remote_copy(
                source, slots.at[o], front_send.at[kind, o], front_recv.at[kind, o],
                device_id=(me, mate), device_id_type=MESH,
            )
            for o, mate in enumerate(mates)
        ]

    token_sends = to_mates(tok, xbuf, 0)
    for copy in token_sends:
        copy.start()
    depth = tok.shape[1]

    def rows_from(weight, o):
        at = pl.multiple_of(lax.rem(t + ways - o, ways) * depth, depth)
        if weight is rdown:
            return weight[:, pl.ds(at, depth)]
        return weight[pl.ds(at, depth), :]

    def project(x, weight, o):
        return dot(x, rows_from(weight, o), ((1,), (1 if weight is rdown else 0,)))

    def rest(value, weight):
        more = project(xbuf[0], weight, 1)
        for o in range(2, ways):
            more = more + project(xbuf[o - 1], weight, o)
        return value + more

    for copy in loads[1:4]:
        copy.wait()
    first = [project(tok[...], weight, 0) for weight in (ldown, qdown, rdown)]
    wides = (inner_w, signal_w, outer_w)
    for i in range(2):
        loads[4 + i].wait()
        early[i] = project(tok[...], wides[i], 0)
    for copy in token_sends:
        copy.wait_recv()
    lat_part, query_part, turn_part = [rest(v, w) for v, w in zip(first, (ldown, qdown, rdown))]
    raw_lat[ways - 1] = lat_part.astype(jnp.bfloat16)
    raw_query[ways - 1] = query_part.astype(jnp.bfloat16)
    latent_sends = to_mates(raw_lat.at[ways - 1], raw_lat, 1) + to_mates(raw_query.at[ways - 1], raw_query, 2)
    for copy in latent_sends:
        copy.start()

    turn = jnp.concatenate([turn_part, jnp.zeros((rows, LANES - ROPE), jnp.float32)], 1).T
    spun = rotated(turn[:ROPE])

    inner = rest(early[0], inner_w)
    signal = rest(early[1], signal_w)
    gated = (inner * signal).astype(jnp.bfloat16)
    padded[EDGE:] = gated.astype(jnp.float32)
    edge[...] = gated[rows - EDGE :]

    def whole(raw, gain_ref):
        values = jnp.concatenate([raw[lax.rem(t + ways - 1 - s, ways)] for s in range(ways)], 1).astype(jnp.float32)
        factor = lax.rsqrt(jnp.mean(values * values, -1, keepdims=True) + norm_epsilon)
        return (values * factor * gain_ref[...]).astype(jnp.bfloat16)

    for copy in latent_sends[: len(mates)]:
        copy.wait_recv()
    latent_norm = whole(raw_lat, lgain_ref)
    wide = kv.shape[3]
    for s in range(ways):
        kv[me, s, :rows] = latent_norm[:, s * wide : (s + 1) * wide]
        kv[me, s, rows:] = spun[:, s * wide : (s + 1) * wide]

    def send(j, target, sem):
        return pltpu.make_async_remote_copy(
            kv.at[j, t], kv.at[j, t], sem, kv_recv.at[j], device_id=(target, t), device_id_type=MESH
        )

    def shares(j):
        return [
            pltpu.make_async_remote_copy(
                kv.at[j, t], kv.at[j, t], share_send.at[j, o], share_recv.at[j, o],
                device_id=(me, mate), device_id_type=MESH,
            )
            for o, mate in enumerate(mates)
        ]

    def landed(j):
        for o in range(len(mates)):
            source = lax.rem(t + ways - 1 - o, ways)
            pltpu.make_async_remote_copy(
                kv.at[j, source], kv.at[j, source], share_send.at[j, o], share_recv.at[j, o],
                device_id=(me, mates[o]), device_id_type=MESH,
            ).wait_recv()

    def collect(j):
        send(j, me, side_send.at[j, 0]).wait_recv()
        for copy in shares(j):
            copy.start()

    def relay(j):
        collect(j)
        for k in range(3):
            send(j, me + cross[k], side_send.at[j, k]).start()

    def own_sends(go):
        for d in range(1, planes):

            @pl.when(z + d < planes)
            def _():
                go(send(me, me + 4 * d, up_send.at[d - 1]))

        for k, bit in enumerate((b0, b1, b1)):

            @pl.when(bit == 0)
            def _():
                go(send(me, me + cross[k], side_send.at[me, k]))

    own_sends(lambda copy: copy.start())
    rim_copy = pltpu.make_async_remote_copy(
        edge, rim, front_send.at[3, 0], front_recv.at[3, 0], device_id=(after, t), device_id_type=MESH
    )

    @pl.when(me + 1 < total)
    def _():
        rim_copy.start()

    loads[6].wait()
    low = lax.broadcasted_iota(jnp.int32, (1, 2 * NOPE), 1) < NOPE
    width = NOPE + VDIM
    for p in range(heads // 2):
        even = up_ref[:, 2 * p * width : (2 * p + 1) * width].astype(jnp.float32)
        odd = up_ref[:, (2 * p + 1) * width : (2 * p + 2) * width].astype(jnp.float32)
        at = slice(p * width, (p + 1) * width)
        wk_ref[:, at] = jnp.where(low, even, pltpu.roll(odd, NOPE, 1)).astype(jnp.bfloat16)
        wvt_ref[at] = jnp.where(low, pltpu.roll(even, NOPE, 1), odd).T.astype(jnp.bfloat16)

    loads[7].wait()
    for copy in latent_sends[len(mates) :]:
        copy.wait_recv()
    scale = (NOPE + ROPE) ** (-0.5) * log2e
    query = (dot(whole(raw_query, qgain_ref), qup[...]) * scale).T
    size = NOPE + ROPE
    for h in range(heads):
        base = h * size
        side = h % 2 * NOPE
        qx_ref[h, side : side + NOPE] = query[base : base + NOPE].astype(jnp.bfloat16)
        qx_ref[h, NOPE - side : 2 * NOPE - side] = jnp.zeros((NOPE, rows), jnp.bfloat16)
        qx_ref[h, 2 * NOPE : 2 * NOPE + ROPE] = rotated(query[base + NOPE : base + size])
        qx_ref[h, 2 * NOPE + ROPE :] = jnp.zeros((LANES - ROPE, rows), jnp.bfloat16)

    def run(blocks, masked):
        lat_parts = []
        rot_parts = []
        for j in blocks:
            lat_parts.append(jnp.concatenate([kv[j, s, :rows] for s in range(ways)], 1))
            spin = jnp.concatenate([kv[j, s, rows:] for s in range(ways)], 1).astype(jnp.float32)
            spin = jnp.concatenate([spin, jnp.zeros((LANES - ROPE, rows), jnp.float32)], 0)
            rot_parts.append(spin.T.astype(jnp.bfloat16))
        unit(
            lat_parts, rot_parts, qx_ref, wk_ref, wvt_ref, keys, turned, scores, weights, best_ref, acc_ref, masked
        )

    run([me], True)
    loads[8].wait()
    outer = rest(project(tok[...], outer_w, 0), outer_w)

    @pl.when(me > 0)
    def _():
        rim_copy.wait_recv()
        padded[:EDGE] = rim[...].astype(jnp.float32)

    @pl.when(me == 0)
    def _():
        padded[:EDGE] = jnp.zeros((EDGE, padded.shape[1]), jnp.float32)

    reach = taps_ref.shape[0] - 1
    taps = taps_ref[...].astype(jnp.float32)
    filtered = padded[EDGE:] * taps[reach : reach + 1, :]
    for k in range(reach):
        filtered = filtered + padded[EDGE - reach + k : EDGE - reach + k + rows] * taps[k : k + 1, :]
    conv_ref[...] = (outer * filtered).astype(jnp.bfloat16)

    @pl.when(b0 == 1)
    def _():
        collect(me + cross[0])

    @pl.when(z > 0)
    def _():
        relay(me - 4)

    loads[9].wait()
    cpart[...] = dot(conv_ref[...], cproj_ref[...])

    @pl.when(b0 == 1)
    def _():
        landed(me + cross[0])
        run([me + cross[0]], False)

    @pl.when(b1 == 1)
    def _():
        collect(me + cross[1])
        collect(me + cross[2])

    @pl.loop(0, 2 * z + 1)
    def _(n):
        plane = (n + 1) // 2
        odd = n % 2
        own = me - 4 * plane

        @pl.when(n + 2 <= z)
        def _():
            relay(own + 4 * plane - 4 * (n + 2))

        @pl.when(n < 2 * z)
        def _():
            then = me - 4 * ((n + 2) // 2)

            @pl.when(odd == 0)
            def _():
                collect(then + cross[0])

            @pl.when(odd == 1)
            def _():
                collect(then + cross[1])
                collect(then + cross[2])

        left = own + (1 - odd) * cross[1]
        right = own + odd * cross[0] + (1 - odd) * cross[2]

        @pl.when(n + b1 > 0)
        def _():
            landed(left)
            landed(right)
            run([left, right], False)

    for h in range(heads):
        acc = acc_ref[h]
        acc_ref[h, :VDIM] = acc[:VDIM] / acc[VDIM : VDIM + 1]
    flat = jnp.concatenate([acc_ref[h, :VDIM] for h in range(heads)], 0)
    att[...] = flat.T.astype(jnp.bfloat16)

    loads[10].wait()

    def part(owner):
        at = pl.ds(pl.multiple_of(owner * short, short), short)
        return (cpart[at, :] + dot(att[at, :], aproj_ref[...])).astype(jnp.bfloat16)

    tails = []
    for o, mate in enumerate(mates):
        part_buf[o] = part(mate)
        tails.append(
            pltpu.make_async_remote_copy(
                part_buf.at[o], in_buf.at[o], tail_send.at[o], tail_recv.at[o],
                device_id=(me, mate), device_id_type=MESH,
            )
        )
        tails[-1].start()
    result = part(t).astype(jnp.float32)
    for o, copy in enumerate(tails):
        copy.wait_recv()
        result = result + in_buf[o].astype(jnp.float32)
    out_ref[...] = result.astype(jnp.bfloat16)
    for copy in tails + token_sends + latent_sends:
        copy.wait_send()

    @pl.when(me + 1 < total)
    def _():
        rim_copy.wait_send()

    own_sends(lambda copy: copy.wait_send())

    @pl.when(b0 == 1)
    def _():
        for copy in shares(me + cross[0]):
            copy.wait_send()

    @pl.when(b1 == 1)
    def _():
        for copy in shares(me + cross[1]) + shares(me + cross[2]):
            copy.wait_send()

    @pl.loop(1, z + 1)
    def _(d):
        j = me - 4 * d
        for k in range(3):
            send(j, me + cross[k], side_send.at[j, k]).wait_send()
        for c in (0,) + cross:
            for copy in shares(j + c):
                copy.wait_send()


def local(
    tokens,
    outer_gate,
    inner_gate,
    conv_input,
    conv_taps,
    query_down,
    latent_down,
    rotary_down,
    query_gain,
    latent_gain,
    query_up,
    latent_up,
    conv_project,
    attend_project,
):
    rows = tokens.shape[0]
    heads = query_up.shape[1] // (NOPE + ROPE)
    ways = lax.axis_size("tp")
    blocks = lax.axis_size("sp")
    model = conv_project.shape[1]
    kvr = latent_up.shape[0]
    channels = conv_project.shape[0]
    half = ROPE // 2
    inverse = jnp.asarray(np.float32(rotary_base) ** (-(np.arange(half, dtype=np.float32) * 2.0 / (2 * half))), jnp.float32)
    vmem = pl.BlockSpec(memory_space=pltpu.VMEM)
    dma = pltpu.SemaphoreType.DMA
    mates = ways - 1
    ring = min(heads, RING)
    big = (
        tokens, latent_down, query_down, rotary_down.T, inner_gate, conv_input,
        latent_up, query_up, outer_gate, conv_project, attend_project,
    )

    def half_type(*shape):
        return pltpu.VMEM(shape, jnp.bfloat16)

    def full_type(*shape):
        return pltpu.VMEM(shape, jnp.float32)

    return pl.pallas_call(
        mix_kernel,
        out_shape=jax.ShapeDtypeStruct((rows // ways, model), jnp.bfloat16),
        in_specs=[pl.BlockSpec(memory_space=pl.ANY)] + [vmem] * 4 + [pl.BlockSpec(memory_space=pl.ANY)] * (len(big) - 1),
        out_specs=vmem,
        scratch_shapes=[half_type(*array.shape) for array in big]
        + [
            half_type(mates, *tokens.shape),
            half_type(ways, rows, latent_down.shape[1]),
            half_type(ways, rows, query_down.shape[1]),
            half_type(EDGE, channels),
            half_type(EDGE, channels),
            full_type(EDGE + rows, channels),
            half_type(rows, channels),
            half_type(kvr, heads * NOPE),
            half_type(heads * VDIM, kvr),
            half_type(heads, 2 * NOPE + LANES, rows),
            half_type(blocks, ways, rows + ROPE, kvr // ways),
            half_type(2 * rows, heads * NOPE),
            half_type(heads, VDIM + ONES, 2 * rows),
            full_type(ring, 2 * rows, rows),
            half_type(ring, 2 * rows, rows),
            full_type(heads, 1, rows),
            full_type(heads, VDIM + ONES, rows),
            half_type(rows, heads * VDIM),
            full_type(2, rows, channels),
            full_type(rows, model),
            half_type(mates, rows // ways, model),
            half_type(mates, rows // ways, model),
            dma((len(big),)),
            dma((4, mates)),
            dma((4, mates)),
            dma((blocks // 4 - 1,)),
            dma((blocks, 3)),
            dma((blocks,)),
            dma((blocks, mates)),
            dma((blocks, mates)),
            dma((mates,)),
            dma((mates,)),
        ],
        compiler_params=pltpu.CompilerParams(
            vmem_limit_bytes=60 * 1024 * 1024, collective_id=0, has_side_effects=True
        ),
    )(
        tokens,
        inverse[:, None],
        conv_taps,
        query_gain[None, :],
        latent_gain[None, :],
        *big[1:],
    )


def solution(mesh):
    split = P(None, "tp")
    in_specs = (P("sp", "tp"),) + (split,) * 6 + (P(),) * 3 + (split,) * 2 + (P("tp", None),) * 2
    out_specs = P(("sp", "tp"), None)
    return jax.shard_map(local, mesh=mesh, in_specs=in_specs, out_specs=out_specs, check_vma=False)
```

```python
import jax
import numpy as np
import jax.numpy as jnp
from jax import lax
from jax.experimental import pallas as pl
from jax.experimental.pallas import tpu as pltpu
from jax.sharding import PartitionSpec as P

NOPE = 64
ROPE = 32
VDIM = 64
LANES = 128
ONES = 16
EDGE = 16
RING = 8
LAG = 2
EAGER = 9

MESH = pl.DeviceIdType.MESH
neg_fill = -1e30
rotary_base = 10000.0
norm_epsilon = 1e-06
log2e = 1.4426950408889634


def dot(a, b, dims=((1,), (0,))):
    return lax.dot_general(a, b, (dims, ((), ())), preferred_element_type=jnp.float32)


def unit(lat_parts, rot_parts, qx_ref, wk_ref, wvt_ref, keys, turned, scores, weights, best_ref, acc_ref, masked):
    heads, _, rows = qx_ref.shape
    latent = jnp.concatenate(lat_parts, 0)
    rot = jnp.concatenate(rot_parts, 0)
    span = latent.shape[0]
    keys[:span] = dot(latent, wk_ref[...]).astype(jnp.bfloat16)
    flat = dot(wvt_ref[...], latent, ((1,), (1,))).astype(jnp.bfloat16)
    for h in range(heads):
        turned[h, :VDIM, :span] = flat[h * VDIM : (h + 1) * VDIM]
    ring = scores.shape[0]
    tops = [None] * heads

    def score(h):
        pair = h // 2 * 2 * NOPE
        key = jnp.concatenate([keys[:span, pair : pair + 2 * NOPE], rot], 1)
        s = dot(key, qx_ref[h])
        if masked:
            k_at = lax.broadcasted_iota(jnp.int32, s.shape, 0)
            q_at = lax.broadcasted_iota(jnp.int32, s.shape, 1)
            s = jnp.where(k_at <= q_at, s, neg_fill)
        scores[h % ring, :span] = s
        top = jnp.max(s, 0, keepdims=True)
        if masked:
            tops[h] = (top, None)
        else:
            old = best_ref[h]
            top = jnp.maximum(old, top)
            tops[h] = (top, jnp.exp2(old - top))
        best_ref[h] = top

    def soften(h):
        weights[h % ring, :span] = jnp.exp2((scores[h % ring, :span] - tops[h][0]).astype(jnp.bfloat16))

    def gather(h):
        fresh = dot(turned[h, :, :span], weights[h % ring, :span])
        acc_ref[h] = fresh if masked else acc_ref[h] * tops[h][1] + fresh

    for step in range(heads + 2 * LAG):
        if step < heads:
            score(step)
        if 0 <= step - LAG < heads:
            soften(step - LAG)
        if 0 <= step - 2 * LAG < heads:
            gather(step - 2 * LAG)


def mix_kernel(
    inv_in, tok_in, ldown_in, rdown_in, qdown_in, up_in, inner_in, signal_in, lgain_in, qgain_in, qup_in, taps_in, outer_in, cproj_in, aproj_in,
    out_ref,
    inv_ref, tok, ldown, rdown, qdown, up_ref, inner_w, signal_w, lgain_ref, qgain_ref, qup, taps_ref, outer_w, cproj_ref, aproj_ref,
    xbuf, raw_lat, raw_query, edge, rim, padded, conv_ref, wk_ref, wvt_ref, qx_ref,
    kv, keys, turned, scores, weights, best_ref, acc_ref, att, small, held, cpart, part_buf, in_buf,
    load_sem, front_send, front_recv, up_send, side_send, kv_recv, share_send, share_recv, tail_send, tail_recv,
):
    me = lax.axis_index("sp")
    t = lax.axis_index("tp")
    total = lax.axis_size("sp")
    ways = lax.axis_size("tp")
    planes = total // 4
    z = me // 4
    b0 = me % 2
    b1 = (me // 2) % 2
    heads, _, rows = qx_ref.shape
    short = rows // ways
    cross = (1 - 2 * b0, 2 - 4 * b1, 3 - 2 * b0 - 4 * b1)
    after = lax.rem(me + 1, total)
    before = lax.rem(me + total - 1, total)
    mates = [lax.rem(t + o, ways) for o in range(1, ways)]

    barrier = pltpu.get_barrier_semaphore()
    targets = [(me, mate) for mate in mates] + [(me + c, t) for c in cross]
    targets += [(lax.rem(me + 4 * d, total), t) for d in range(1, planes)] + [(after, t), (before, t)]
    for target in targets:
        pl.semaphore_signal(barrier, inc=1, device_id=target, device_id_type=MESH)

    pairs = (
        (tok_in, tok), (ldown_in, ldown), (rdown_in, rdown), (qdown_in, qdown), (inv_in, inv_ref),
        (lgain_in, lgain_ref), (qgain_in, qgain_ref), (taps_in, taps_ref), (inner_in, inner_w), (up_in, up_ref),
        (qup_in, qup), (signal_in, signal_w), (outer_in, outer_w), (cproj_in, cproj_ref), (aproj_in, aproj_ref),
    )
    loads = [pltpu.make_async_copy(a, b, load_sem.at[i]) for i, (a, b) in enumerate(pairs)]
    for copy in loads[:EAGER]:
        copy.start()

    pl.semaphore_wait(barrier, len(targets))
    loads[0].wait()

    def to_mates(source, slots, kind):
        return [
            pltpu.make_async_remote_copy(
                source, slots.at[o], front_send.at[kind, o], front_recv.at[kind, o],
                device_id=(me, mate), device_id_type=MESH,
            )
            for o, mate in enumerate(mates)
        ]

    token_sends = to_mates(tok, xbuf, 0)
    for copy in token_sends:
        copy.start()
    loads[4].wait()
    position = (me * rows + lax.broadcasted_iota(jnp.int32, (1, rows), 1)).astype(jnp.float32)
    angle = inv_ref[...] * position
    cosine = jnp.cos(angle)
    sine = jnp.sin(angle)
    half = ROPE // 2

    def rotated(values):
        a = values[:half]
        b = values[half:]
        return jnp.concatenate([a * cosine - b * sine, a * sine + b * cosine], 0).astype(jnp.bfloat16)

    for h in range(heads):
        turned[h, VDIM:] = jnp.ones((ONES, turned.shape[2]), jnp.bfloat16)
    depth = tok.shape[1]

    def rows_from(weight, o):
        at = pl.multiple_of(lax.rem(t + ways - o, ways) * depth, depth)
        if weight is rdown:
            return weight[:, pl.ds(at, depth)]
        return weight[pl.ds(at, depth), :]

    def project(x, weight, o):
        return dot(x, rows_from(weight, o), ((1,), (1 if weight is rdown else 0,)))

    def rest(value, weight):
        more = project(xbuf[0], weight, 1)
        for o in range(2, ways):
            more = more + project(xbuf[o - 1], weight, o)
        return value + more

    for copy in loads[1:4]:
        copy.wait()
    for copy in loads[EAGER:]:
        copy.start()
    narrow = (ldown, qdown, rdown)
    spots = []
    for weight in narrow:
        start = spots[-1].stop if spots else 0
        spots.append(slice(start, start + (LANES if weight is rdown else weight.shape[1])))
    for weight, spot in zip(narrow, spots):
        small[:, spot.start : spot.start + (ROPE if weight is rdown else weight.shape[1])] = project(tok[...], weight, 0)
    for copy in token_sends:
        copy.wait_recv()
    raw_lat[ways - 1] = rest(small[:, spots[0]], ldown).astype(jnp.bfloat16)
    latent_sends = to_mates(raw_lat.at[ways - 1], raw_lat, 1)
    query_sends = to_mates(raw_query.at[ways - 1], raw_query, 2)
    for copy in latent_sends:
        copy.start()
    raw_query[ways - 1] = rest(small[:, spots[1]], qdown).astype(jnp.bfloat16)
    for copy in query_sends:
        copy.start()
    turn_part = rest(small[:, spots[2].start : spots[2].start + ROPE], rdown)
    turn = jnp.concatenate([turn_part, jnp.zeros((rows, LANES - ROPE), jnp.float32)], 1).T
    spun = rotated(turn[:ROPE])

    loads[8].wait()
    held[...] = rest(project(tok[...], inner_w, 0), inner_w)

    def whole(raw, gain_ref):
        values = jnp.concatenate([raw[lax.rem(t + ways - 1 - s, ways)] for s in range(ways)], 1).astype(jnp.float32)
        factor = lax.rsqrt(jnp.mean(values * values, -1, keepdims=True) + norm_epsilon)
        return (values * factor * gain_ref[...]).astype(jnp.bfloat16)

    for copy in latent_sends:
        copy.wait_recv()
    loads[5].wait()
    latent_norm = whole(raw_lat, lgain_ref)
    wide = kv.shape[3]
    for s in range(ways):
        kv[me, s, :rows] = latent_norm[:, s * wide : (s + 1) * wide]
        kv[me, s, rows:] = spun[:, s * wide : (s + 1) * wide]

    def send(j, target, sem):
        return pltpu.make_async_remote_copy(
            kv.at[j, t], kv.at[j, t], sem, kv_recv.at[j], device_id=(target, t), device_id_type=MESH
        )

    def shares(j):
        return [
            pltpu.make_async_remote_copy(
                kv.at[j, t], kv.at[j, t], share_send.at[j, o], share_recv.at[j, o],
                device_id=(me, mate), device_id_type=MESH,
            )
            for o, mate in enumerate(mates)
        ]

    def landed(j):
        for o in range(len(mates)):
            source = lax.rem(t + ways - 1 - o, ways)
            pltpu.make_async_remote_copy(
                kv.at[j, source], kv.at[j, source], share_send.at[j, o], share_recv.at[j, o],
                device_id=(me, mates[o]), device_id_type=MESH,
            ).wait_recv()

    def collect(j):
        send(j, me, side_send.at[j, 0]).wait_recv()
        for copy in shares(j):
            copy.start()

    def lift(d, go):
        j = me - 4 * d

        @pl.when(jnp.logical_and(d % 3 < 2, z + 1 < planes))
        def _():
            go(send(j, me + 4, up_send.at[j, 0]))

        @pl.when(jnp.logical_and(d % 3 == 0, z + 3 < planes))
        def _():
            go(send(j, me + 12, up_send.at[j, 1]))

    def relay(d):
        j = me - 4 * d
        send(j, me, side_send.at[j, 0]).wait_recv()
        lift(d, lambda copy: copy.start())
        for k in range(3):
            send(j, me + cross[k], side_send.at[j, k]).start()
        for copy in shares(j):
            copy.start()

    def own_sends(go):
        lift(0, go)
        for k, bit in enumerate((b0, b1, b1)):

            @pl.when(bit == 0)
            def _():
                go(send(me, me + cross[k], side_send.at[me, k]))

    own_sends(lambda copy: copy.start())
    loads[9].wait()
    low = lax.broadcasted_iota(jnp.int32, (1, 2 * NOPE), 1) < NOPE
    width = NOPE + VDIM
    for p in range(heads // 2):
        even = up_ref[:, 2 * p * width : (2 * p + 1) * width].astype(jnp.float32)
        odd = up_ref[:, (2 * p + 1) * width : (2 * p + 2) * width].astype(jnp.float32)
        at = slice(p * width, (p + 1) * width)
        wk_ref[:, at] = jnp.where(low, even, pltpu.roll(odd, NOPE, 1)).astype(jnp.bfloat16)
        wvt_ref[at] = jnp.where(low, pltpu.roll(even, NOPE, 1), odd).T.astype(jnp.bfloat16)

    loads[6].wait()
    loads[10].wait()
    for copy in query_sends:
        copy.wait_recv()
    scale = (NOPE + ROPE) ** (-0.5) * log2e
    query = (dot(whole(raw_query, qgain_ref), qup[...]) * scale).T
    size = NOPE + ROPE
    for h in range(heads):
        base = h * size
        side = h % 2 * NOPE
        qx_ref[h, side : side + NOPE] = query[base : base + NOPE].astype(jnp.bfloat16)
        qx_ref[h, NOPE - side : 2 * NOPE - side] = jnp.zeros((NOPE, rows), jnp.bfloat16)
        qx_ref[h, 2 * NOPE : 2 * NOPE + ROPE] = rotated(query[base + NOPE : base + size])
        qx_ref[h, 2 * NOPE + ROPE :] = jnp.zeros((LANES - ROPE, rows), jnp.bfloat16)

    def run(blocks, masked):
        lat_parts = []
        rot_parts = []
        for j in blocks:
            lat_parts.append(jnp.concatenate([kv[j, s, :rows] for s in range(ways)], 1))
            spin = jnp.concatenate([kv[j, s, rows:] for s in range(ways)], 1).astype(jnp.float32)
            spin = jnp.concatenate([spin, jnp.zeros((LANES - ROPE, rows), jnp.float32)], 0)
            rot_parts.append(spin.T.astype(jnp.bfloat16))
        unit(
            lat_parts, rot_parts, qx_ref, wk_ref, wvt_ref, keys, turned, scores, weights, best_ref, acc_ref, masked
        )

    run([me], True)
    loads[11].wait()
    signal = rest(project(tok[...], signal_w, 0), signal_w)
    gated = (held[...] * signal).astype(jnp.bfloat16)
    padded[EDGE:] = gated.astype(jnp.float32)
    edge[...] = gated[rows - EDGE :]
    rim_copy = pltpu.make_async_remote_copy(
        edge, rim, front_send.at[3, 0], front_recv.at[3, 0], device_id=(after, t), device_id_type=MESH
    )

    @pl.when(me + 1 < total)
    def _():
        rim_copy.start()

    loads[12].wait()
    held[...] = rest(project(tok[...], outer_w, 0), outer_w)

    @pl.when(z > 0)
    def _():
        relay(1)

    @pl.when(b0 == 1)
    def _():
        collect(me + cross[0])
        landed(me + cross[0])
        run([me + cross[0]], False)

    @pl.when(b1 == 1)
    def _():
        collect(me + cross[1])
        collect(me + cross[2])

    loads[7].wait()

    @pl.when(me > 0)
    def _():
        rim_copy.wait_recv()
        padded[:EDGE] = rim[...].astype(jnp.float32)

    @pl.when(me == 0)
    def _():
        padded[:EDGE] = jnp.zeros((EDGE, padded.shape[1]), jnp.float32)

    reach = taps_ref.shape[0] - 1
    taps = taps_ref[...].astype(jnp.float32)
    filtered = padded[EDGE:] * taps[reach : reach + 1, :]
    for k in range(reach):
        filtered = filtered + padded[EDGE - reach + k : EDGE - reach + k + rows] * taps[k : k + 1, :]
    conv_ref[...] = (held[...] * filtered).astype(jnp.bfloat16)

    loads[13].wait()
    cpart[...] = dot(conv_ref[...], cproj_ref[...])

    @pl.loop(0, 2 * z + 1)
    def _(n):
        plane = (n + 1) // 2
        odd = n % 2
        own = me - 4 * plane

        @pl.when(n + 2 <= z)
        def _():
            relay(n + 2)

        @pl.when(n < 2 * z)
        def _():
            then = me - 4 * ((n + 2) // 2)

            @pl.when(odd == 0)
            def _():
                collect(then + cross[0])

            @pl.when(odd == 1)
            def _():
                collect(then + cross[1])
                collect(then + cross[2])

        left = own + (1 - odd) * cross[1]
        right = own + odd * cross[0] + (1 - odd) * cross[2]

        @pl.when(n + b1 > 0)
        def _():
            landed(left)
            landed(right)
            run([left, right], False)

    for h in range(heads):
        acc = acc_ref[h]
        acc_ref[h, :VDIM] = acc[:VDIM] / acc[VDIM : VDIM + 1]
    flat = jnp.concatenate([acc_ref[h, :VDIM] for h in range(heads)], 0)
    att[...] = flat.T.astype(jnp.bfloat16)

    loads[14].wait()

    def part(owner):
        at = pl.ds(pl.multiple_of(owner * short, short), short)
        return (cpart[at, :] + dot(att[at, :], aproj_ref[...])).astype(jnp.bfloat16)

    tails = []
    for o, mate in enumerate(mates):
        part_buf[o] = part(mate)
        tails.append(
            pltpu.make_async_remote_copy(
                part_buf.at[o], in_buf.at[o], tail_send.at[o], tail_recv.at[o],
                device_id=(me, mate), device_id_type=MESH,
            )
        )
        tails[-1].start()
    result = part(t).astype(jnp.float32)
    for o, copy in enumerate(tails):
        copy.wait_recv()
        result = result + in_buf[o].astype(jnp.float32)
    out_ref[...] = result.astype(jnp.bfloat16)
    for copy in tails + token_sends + latent_sends + query_sends:
        copy.wait_send()

    @pl.when(me + 1 < total)
    def _():
        rim_copy.wait_send()

    own_sends(lambda copy: copy.wait_send())

    @pl.when(b0 == 1)
    def _():
        for copy in shares(me + cross[0]):
            copy.wait_send()

    @pl.when(b1 == 1)
    def _():
        for copy in shares(me + cross[1]) + shares(me + cross[2]):
            copy.wait_send()

    @pl.loop(1, z + 1)
    def _(d):
        j = me - 4 * d
        lift(d, lambda copy: copy.wait_send())
        for k in range(3):
            send(j, me + cross[k], side_send.at[j, k]).wait_send()
        for c in (0,) + cross:
            for copy in shares(j + c):
                copy.wait_send()


def local(
    tokens,
    outer_gate,
    inner_gate,
    conv_input,
    conv_taps,
    query_down,
    latent_down,
    rotary_down,
    query_gain,
    latent_gain,
    query_up,
    latent_up,
    conv_project,
    attend_project,
):
    rows = tokens.shape[0]
    heads = query_up.shape[1] // (NOPE + ROPE)
    ways = lax.axis_size("tp")
    blocks = lax.axis_size("sp")
    model = conv_project.shape[1]
    kvr = latent_up.shape[0]
    channels = conv_project.shape[0]
    half = ROPE // 2
    inverse = jnp.asarray(np.float32(rotary_base) ** (-(np.arange(half, dtype=np.float32) * 2.0 / (2 * half))), jnp.float32)
    vmem = pl.BlockSpec(memory_space=pltpu.VMEM)
    dma = pltpu.SemaphoreType.DMA
    mates = ways - 1
    ring = min(heads, RING)
    big = (
        inverse[:, None], tokens, latent_down, rotary_down.T, query_down, latent_up, inner_gate, conv_input,
        latent_gain[None, :], query_gain[None, :], query_up, conv_taps, outer_gate, conv_project, attend_project,
    )

    def half_type(*shape):
        return pltpu.VMEM(shape, jnp.bfloat16)

    def full_type(*shape):
        return pltpu.VMEM(shape, jnp.float32)

    return pl.pallas_call(
        mix_kernel,
        out_shape=pltpu.VMEM((rows // ways, model), jnp.bfloat16),
        in_specs=[pl.BlockSpec(memory_space=pl.ANY)] * len(big),
        out_specs=vmem,
        scratch_shapes=[pltpu.VMEM(array.shape, array.dtype) for array in big]
        + [
            half_type(mates, *tokens.shape),
            half_type(ways, rows, latent_down.shape[1]),
            half_type(ways, rows, query_down.shape[1]),
            half_type(EDGE, channels),
            half_type(EDGE, channels),
            full_type(EDGE + rows, channels),
            half_type(rows, channels),
            half_type(kvr, heads * NOPE),
            half_type(heads * VDIM, kvr),
            half_type(heads, 2 * NOPE + LANES, rows),
            half_type(blocks, ways, rows + ROPE, kvr // ways),
            half_type(2 * rows, heads * NOPE),
            half_type(heads, VDIM + ONES, 2 * rows),
            full_type(ring, 2 * rows, rows),
            half_type(ring, 2 * rows, rows),
            full_type(heads, 1, rows),
            full_type(heads, VDIM + ONES, rows),
            half_type(rows, heads * VDIM),
            full_type(rows, latent_down.shape[1] + query_down.shape[1] + LANES),
            full_type(rows, channels),
            full_type(rows, model),
            half_type(mates, rows // ways, model),
            half_type(mates, rows // ways, model),
            dma((len(big),)),
            dma((4, mates)),
            dma((4, mates)),
            dma((blocks, 2)),
            dma((blocks, 3)),
            dma((blocks,)),
            dma((blocks, mates)),
            dma((blocks, mates)),
            dma((mates,)),
            dma((mates,)),
        ],
        compiler_params=pltpu.CompilerParams(
            vmem_limit_bytes=60 * 1024 * 1024, collective_id=0, has_side_effects=True
        ),
    )(*big)


def solution(mesh):
    split = P(None, "tp")
    in_specs = (P("sp", "tp"),) + (split,) * 6 + (P(),) * 3 + (split,) * 2 + (P("tp", None),) * 2
    out_specs = P(("sp", "tp"), None)
    return jax.shard_map(local, mesh=mesh, in_specs=in_specs, out_specs=out_specs, check_vma=False)
```

```python
import jax
import numpy as np
import jax.numpy as jnp
from jax import lax
from jax.experimental import pallas as pl
from jax.experimental.pallas import tpu as pltpu
from jax.sharding import PartitionSpec as P

NOPE = 64
ROPE = 32
VDIM = 64
LANES = 128
ONES = 16
EDGE = 16
RING = 8
LAG = 2
EAGER = 9
CHUNKS = 2

MESH = pl.DeviceIdType.MESH
neg_fill = -1e30
rotary_base = 10000.0
norm_epsilon = 1e-06
log2e = 1.4426950408889634


def dot(a, b, dims=((1,), (0,))):
    return lax.dot_general(a, b, (dims, ((), ())), preferred_element_type=jnp.float32)


def unit(lat_parts, rot_parts, qx_ref, wk_ref, wvt_ref, keys, turned, scores, weights, best_ref, acc_ref, masked):
    heads, _, rows = qx_ref.shape
    latent = jnp.concatenate(lat_parts, 0)
    rot = jnp.concatenate(rot_parts, 0)
    span = latent.shape[0]
    keys[:span] = dot(latent, wk_ref[...]).astype(jnp.bfloat16)
    flat = dot(wvt_ref[...], latent, ((1,), (1,))).astype(jnp.bfloat16)
    for h in range(heads):
        turned[h, :VDIM, :span] = flat[h * VDIM : (h + 1) * VDIM]
    ring = scores.shape[0]
    tops = [None] * heads

    def score(h):
        pair = h // 2 * 2 * NOPE
        key = jnp.concatenate([keys[:span, pair : pair + 2 * NOPE], rot], 1)
        s = dot(key, qx_ref[h])
        if masked:
            k_at = lax.broadcasted_iota(jnp.int32, s.shape, 0)
            q_at = lax.broadcasted_iota(jnp.int32, s.shape, 1)
            s = jnp.where(k_at <= q_at, s, neg_fill)
        scores[h % ring, :span] = s
        top = jnp.max(s, 0, keepdims=True)
        if masked:
            tops[h] = (top, None)
        else:
            old = best_ref[h]
            top = jnp.maximum(old, top)
            tops[h] = (top, jnp.exp2(old - top))
        best_ref[h] = top

    def soften(h):
        weights[h % ring, :span] = jnp.exp2((scores[h % ring, :span] - tops[h][0]).astype(jnp.bfloat16))

    def gather(h):
        fresh = dot(turned[h, :, :span], weights[h % ring, :span])
        acc_ref[h] = fresh if masked else acc_ref[h] * tops[h][1] + fresh

    for step in range(heads + 2 * LAG):
        if step < heads:
            score(step)
        if 0 <= step - LAG < heads:
            soften(step - LAG)
        if 0 <= step - 2 * LAG < heads:
            gather(step - 2 * LAG)


def mix_kernel(
    inv_in, tok_in, ldown_in, rdown_in, qdown_in, up_in, inner_in, signal_in, lgain_in, qgain_in, qup_in, taps_in, outer_in, cproj_in, aproj_in,
    out_ref,
    inv_ref, tok, ldown, rdown, qdown, up_ref, inner_w, signal_w, lgain_ref, qgain_ref, qup, taps_ref, outer_w, cproj_ref, aproj_ref,
    xbuf, raw_lat, raw_query, edge, rim, padded, conv_ref, wk_ref, wvt_ref, qx_ref,
    kv, keys, turned, scores, weights, best_ref, acc_ref, att, small, held, cpart, part_buf, in_buf,
    load_sem, front_send, front_recv, up_send, side_send, kv_recv, share_send, share_recv, tail_send, tail_recv,
):
    me = lax.axis_index("sp")
    t = lax.axis_index("tp")
    total = lax.axis_size("sp")
    ways = lax.axis_size("tp")
    planes = total // 4
    z = me // 4
    b0 = me % 2
    b1 = (me // 2) % 2
    heads, _, rows = qx_ref.shape
    short = rows // ways
    cross = (1 - 2 * b0, 2 - 4 * b1, 3 - 2 * b0 - 4 * b1)
    after = lax.rem(me + 1, total)
    before = lax.rem(me + total - 1, total)
    mates = [lax.rem(t + o, ways) for o in range(1, ways)]

    barrier = pltpu.get_barrier_semaphore()
    targets = [(me, mate) for mate in mates] + [(me + c, t) for c in cross]
    targets += [(lax.rem(me + 4 * d, total), t) for d in range(1, planes)] + [(after, t), (before, t)]
    for target in targets:
        pl.semaphore_signal(barrier, inc=1, device_id=target, device_id_type=MESH)

    pairs = (
        (tok_in, tok), (ldown_in, ldown), (rdown_in, rdown), (qdown_in, qdown), (inv_in, inv_ref),
        (lgain_in, lgain_ref), (qgain_in, qgain_ref), (taps_in, taps_ref), (inner_in, inner_w), (up_in, up_ref),
        (qup_in, qup), (signal_in, signal_w), (outer_in, outer_w), (cproj_in, cproj_ref), (aproj_in, aproj_ref),
    )
    loads = [pltpu.make_async_copy(a, b, load_sem.at[i]) for i, (a, b) in enumerate(pairs)]
    for copy in loads[:EAGER]:
        copy.start()

    pl.semaphore_wait(barrier, len(targets))
    loads[0].wait()

    def to_mates(source, slots, kind):
        return [
            pltpu.make_async_remote_copy(
                source, slots.at[o], front_send.at[kind, o], front_recv.at[kind, o],
                device_id=(me, mate), device_id_type=MESH,
            )
            for o, mate in enumerate(mates)
        ]

    token_sends = to_mates(tok, xbuf, 0)
    for copy in token_sends:
        copy.start()
    loads[4].wait()
    position = (me * rows + lax.broadcasted_iota(jnp.int32, (1, rows), 1)).astype(jnp.float32)
    angle = inv_ref[...] * position
    cosine = jnp.cos(angle)
    sine = jnp.sin(angle)
    half = ROPE // 2

    def rotated(values):
        a = values[:half]
        b = values[half:]
        return jnp.concatenate([a * cosine - b * sine, a * sine + b * cosine], 0).astype(jnp.bfloat16)

    for h in range(heads):
        turned[h, VDIM:] = jnp.ones((ONES, turned.shape[2]), jnp.bfloat16)
    depth = tok.shape[1]

    def rows_from(weight, o):
        at = pl.multiple_of(lax.rem(t + ways - o, ways) * depth, depth)
        if weight is rdown:
            return weight[:, pl.ds(at, depth)]
        return weight[pl.ds(at, depth), :]

    def project(x, weight, o):
        return dot(x, rows_from(weight, o), ((1,), (1 if weight is rdown else 0,)))

    def rest(value, weight):
        more = project(xbuf[0], weight, 1)
        for o in range(2, ways):
            more = more + project(xbuf[o - 1], weight, o)
        return value + more

    for copy in loads[1:4]:
        copy.wait()
    for copy in loads[EAGER:]:
        copy.start()
    narrow = (ldown, qdown, rdown)
    spots = []
    for weight in narrow:
        start = spots[-1].stop if spots else 0
        spots.append(slice(start, start + (LANES if weight is rdown else weight.shape[1])))
    for weight, spot in zip(narrow, spots):
        small[:, spot.start : spot.start + (ROPE if weight is rdown else weight.shape[1])] = project(tok[...], weight, 0)
    for copy in token_sends:
        copy.wait_recv()
    raw_lat[ways - 1] = rest(small[:, spots[0]], ldown).astype(jnp.bfloat16)
    latent_sends = to_mates(raw_lat.at[ways - 1], raw_lat, 1)
    query_sends = to_mates(raw_query.at[ways - 1], raw_query, 2)
    for copy in latent_sends:
        copy.start()
    raw_query[ways - 1] = rest(small[:, spots[1]], qdown).astype(jnp.bfloat16)
    for copy in query_sends:
        copy.start()
    turn_part = rest(small[:, spots[2].start : spots[2].start + ROPE], rdown)
    turn = jnp.concatenate([turn_part, jnp.zeros((rows, LANES - ROPE), jnp.float32)], 1).T
    spun = rotated(turn[:ROPE])


    def whole(raw, gain_ref):
        values = jnp.concatenate([raw[lax.rem(t + ways - 1 - s, ways)] for s in range(ways)], 1).astype(jnp.float32)
        factor = lax.rsqrt(jnp.mean(values * values, -1, keepdims=True) + norm_epsilon)
        return (values * factor * gain_ref[...]).astype(jnp.bfloat16)

    for copy in latent_sends:
        copy.wait_recv()
    loads[5].wait()
    latent_norm = whole(raw_lat, lgain_ref)
    wide = kv.shape[3]
    for s in range(ways):
        kv[me, s, :rows] = latent_norm[:, s * wide : (s + 1) * wide]
        kv[me, s, rows:] = spun[:, s * wide : (s + 1) * wide]

    def send(j, target, sem):
        return pltpu.make_async_remote_copy(
            kv.at[j, t], kv.at[j, t], sem, kv_recv.at[j], device_id=(target, t), device_id_type=MESH
        )

    def shares(j):
        return [
            pltpu.make_async_remote_copy(
                kv.at[j, t], kv.at[j, t], share_send.at[j, o], share_recv.at[j, o],
                device_id=(me, mate), device_id_type=MESH,
            )
            for o, mate in enumerate(mates)
        ]

    def landed(j):
        for o in range(len(mates)):
            source = lax.rem(t + ways - 1 - o, ways)
            pltpu.make_async_remote_copy(
                kv.at[j, source], kv.at[j, source], share_send.at[j, o], share_recv.at[j, o],
                device_id=(me, mates[o]), device_id_type=MESH,
            ).wait_recv()

    def arrive(j):
        send(j, me, side_send.at[0, 0]).wait_recv()

    def collect(j):
        arrive(j)
        for copy in shares(j):
            copy.start()

    def lift(d, go, steps):
        for step in steps:
            starts = d % 4 == 0 if step > 1 else jnp.logical_or(d % 4 == 0, d % 4 == 3)

            @pl.when(jnp.logical_and(starts, z + step < planes))
            def _():
                go(send(me - 4 * d, me + 4 * step, up_send.at[d, step - 1]))

    def pass_on(d, ks):
        for k in ks:
            send(me - 4 * d, me + cross[k], side_send.at[d, k]).start()

    def relay(d, ks=(0, 1, 2)):
        j = me - 4 * d
        arrive(j)
        lift(d, begin, (1, 2, 3))
        pass_on(d, ks)
        for copy in shares(j):
            copy.start()

    def begin(copy):
        copy.start()

    def finish(copy):
        copy.wait_send()

    def own_side(go, ks):
        for k in ks:

            @pl.when((b0, b1, b1)[k] == 0)
            def _():
                go(send(me, me + cross[k], side_send.at[0, k]))

    lift(0, begin, (1,))
    own_side(begin, (0, 1))
    loads[9].wait()
    low = lax.broadcasted_iota(jnp.int32, (1, 2 * NOPE), 1) < NOPE
    width = NOPE + VDIM
    for p in range(heads // 2):
        even = up_ref[:, 2 * p * width : (2 * p + 1) * width].astype(jnp.float32)
        odd = up_ref[:, (2 * p + 1) * width : (2 * p + 2) * width].astype(jnp.float32)
        at = slice(p * width, (p + 1) * width)
        wk_ref[:, at] = jnp.where(low, even, pltpu.roll(odd, NOPE, 1)).astype(jnp.bfloat16)
        wvt_ref[at] = jnp.where(low, pltpu.roll(even, NOPE, 1), odd).T.astype(jnp.bfloat16)

    loads[6].wait()
    loads[10].wait()
    for copy in query_sends:
        copy.wait_recv()
    scale = (NOPE + ROPE) ** (-0.5) * log2e
    query = (dot(whole(raw_query, qgain_ref), qup[...]) * scale).T
    size = NOPE + ROPE
    for h in range(heads):
        base = h * size
        side = h % 2 * NOPE
        qx_ref[h, side : side + NOPE] = query[base : base + NOPE].astype(jnp.bfloat16)
        qx_ref[h, NOPE - side : 2 * NOPE - side] = jnp.zeros((NOPE, rows), jnp.bfloat16)
        qx_ref[h, 2 * NOPE : 2 * NOPE + ROPE] = rotated(query[base + NOPE : base + size])
        qx_ref[h, 2 * NOPE + ROPE :] = jnp.zeros((LANES - ROPE, rows), jnp.bfloat16)

    def run(blocks, masked):
        lat_parts = []
        rot_parts = []
        for j in blocks:
            lat_parts.append(jnp.concatenate([kv[j, s, :rows] for s in range(ways)], 1))
            spin = jnp.concatenate([kv[j, s, rows:] for s in range(ways)], 1).astype(jnp.float32)
            spin = jnp.concatenate([spin, jnp.zeros((LANES - ROPE, rows), jnp.float32)], 0)
            rot_parts.append(spin.T.astype(jnp.bfloat16))
        unit(
            lat_parts, rot_parts, qx_ref, wk_ref, wvt_ref, keys, turned, scores, weights, best_ref, acc_ref, masked
        )

    lift(0, begin, (2,))
    own_side(begin, (2,))
    run([me], True)
    lift(0, begin, (3,))
    loads[8].wait()
    inner = rest(project(tok[...], inner_w, 0), inner_w)
    loads[11].wait()
    signal = rest(project(tok[...], signal_w, 0), signal_w)
    gated = (inner * signal).astype(jnp.bfloat16)
    padded[EDGE:] = gated.astype(jnp.float32)
    edge[...] = gated[rows - EDGE :]
    rim_copy = pltpu.make_async_remote_copy(
        edge, rim, front_send.at[3, 0], front_recv.at[3, 0], device_id=(after, t), device_id_type=MESH
    )

    @pl.when(me + 1 < total)
    def _():
        rim_copy.start()

    @pl.when(z > 0)
    def _():
        relay(1, (0, 1))

    loads[12].wait()
    held[...] = rest(project(tok[...], outer_w, 0), outer_w)

    @pl.when(z > 0)
    def _():
        pass_on(1, (2,))


    @pl.when(b0 == 1)
    def _():
        collect(me + cross[0])
        landed(me + cross[0])
        run([me + cross[0]], False)

    @pl.when(b1 == 1)
    def _():
        collect(me + cross[1])
        collect(me + cross[2])

    def convolve():
        loads[7].wait()

        @pl.when(me > 0)
        def _():
            rim_copy.wait_recv()
            padded[:EDGE] = rim[...].astype(jnp.float32)

        @pl.when(me == 0)
        def _():
            padded[:EDGE] = jnp.zeros((EDGE, padded.shape[1]), jnp.float32)

        reach = taps_ref.shape[0] - 1
        taps = taps_ref[...].astype(jnp.float32)
        filtered = padded[EDGE:] * taps[reach : reach + 1, :]
        for k in range(reach):
            filtered = filtered + padded[EDGE - reach + k : EDGE - reach + k + rows] * taps[k : k + 1, :]
        conv_ref[...] = (held[...] * filtered).astype(jnp.bfloat16)

        loads[13].wait()
        cpart[...] = dot(conv_ref[...], cproj_ref[...])

    @pl.loop(0, 2 * z + 1)
    def _(n):
        plane = (n + 1) // 2
        odd = n % 2
        own = me - 4 * plane

        def ahead(when):
            then = me - 4 * ((n + 2) // 2)

            @pl.when(jnp.logical_and(when, jnp.logical_and(n < 2 * z, odd == 0)))
            def _():
                collect(then + cross[0])

            @pl.when(jnp.logical_and(when, jnp.logical_and(n < 2 * z, odd == 1)))
            def _():
                collect(then + cross[1])
                collect(then + cross[2])

        @pl.when(jnp.logical_and(n == 0, b1 == 1))
        def _():
            convolve()

        late = jnp.logical_and(n == 1, b1 == 0)
        ahead(jnp.logical_not(late))
        far = (n + b1) // 2 + 2

        @pl.when(jnp.logical_and(jnp.logical_or(n == 0, (n + b1) % 2 == 0), far <= z))
        def _():
            relay(far)

        @pl.when(jnp.logical_and(n == 0, b1 == 0))
        def _():
            convolve()

        left = own + (1 - odd) * cross[1]
        right = own + odd * cross[0] + (1 - odd) * cross[2]

        @pl.when(n + b1 > 0)
        def _():
            landed(left)
            landed(right)
            run([left, right], False)

        ahead(late)

    loads[14].wait()

    def settle(at):
        flat = []
        for h in range(heads):
            acc = acc_ref[h, :, at]
            flat.append(acc[:VDIM] / acc[VDIM : VDIM + 1])
        return jnp.concatenate(flat, 0).T.astype(jnp.bfloat16)

    if short % LANES:
        att[...] = settle(slice(None))

    model = cpart.shape[1]
    step = model // CHUNKS

    def rows_of(owner):
        at = pl.ds(pl.multiple_of(owner * short, short), short)
        return at, (att[at, :] if short % LANES else settle(at))

    def part(at, mixed, c):
        cols = slice(c * step, (c + 1) * step)
        return (cpart[at, cols] + dot(mixed, aproj_ref[:, cols])).astype(jnp.bfloat16)

    tails = []
    for o, mate in enumerate(mates):
        at, mixed = rows_of(mate)
        for c in range(CHUNKS):
            cols = pl.ds(c * step, step)
            part_buf[o, :, cols] = part(at, mixed, c)
            tails.append(
                pltpu.make_async_remote_copy(
                    part_buf.at[o, :, cols], in_buf.at[o, :, cols], tail_send.at[o, c], tail_recv.at[o, c],
                    device_id=(me, mate), device_id_type=MESH,
                )
            )
            tails[-1].start()
    at, mixed = rows_of(t)
    for c in range(CHUNKS):
        cpart[:short, c * step : (c + 1) * step] = part(at, mixed, c).astype(jnp.float32)
    for c in range(CHUNKS):
        cols = slice(c * step, (c + 1) * step)
        result = cpart[:short, cols]
        for o in range(len(mates)):
            tails[o * CHUNKS + c].wait_recv()
            result = result + in_buf[o, :, cols].astype(jnp.float32)
        out_ref[:, cols] = result.astype(jnp.bfloat16)
    for copy in tails + token_sends + latent_sends + query_sends:
        copy.wait_send()

    @pl.when(me + 1 < total)
    def _():
        rim_copy.wait_send()

    lift(0, finish, (1, 2, 3))
    own_side(finish, (0, 1, 2))

    @pl.when(b0 == 1)
    def _():
        for copy in shares(me + cross[0]):
            copy.wait_send()

    @pl.when(b1 == 1)
    def _():
        for copy in shares(me + cross[1]) + shares(me + cross[2]):
            copy.wait_send()

    @pl.loop(1, z + 1)
    def _(d):
        j = me - 4 * d
        lift(d, finish, (1, 2, 3))
        for k in range(3):
            send(j, me + cross[k], side_send.at[d, k]).wait_send()
        for c in (0,) + cross:
            for copy in shares(j + c):
                copy.wait_send()


def local(
    tokens,
    outer_gate,
    inner_gate,
    conv_input,
    conv_taps,
    query_down,
    latent_down,
    rotary_down,
    query_gain,
    latent_gain,
    query_up,
    latent_up,
    conv_project,
    attend_project,
):
    rows = tokens.shape[0]
    heads = query_up.shape[1] // (NOPE + ROPE)
    ways = lax.axis_size("tp")
    blocks = lax.axis_size("sp")
    model = conv_project.shape[1]
    kvr = latent_up.shape[0]
    channels = conv_project.shape[0]
    half = ROPE // 2
    inverse = jnp.asarray(np.float32(rotary_base) ** (-(np.arange(half, dtype=np.float32) * 2.0 / (2 * half))), jnp.float32)
    vmem = pl.BlockSpec(memory_space=pltpu.VMEM)
    dma = pltpu.SemaphoreType.DMA
    mates = ways - 1
    ring = min(heads, RING)
    big = (
        inverse[:, None], tokens, latent_down, rotary_down.T, query_down, latent_up, inner_gate, conv_input,
        latent_gain[None, :], query_gain[None, :], query_up, conv_taps, outer_gate, conv_project, attend_project,
    )

    def half_type(*shape):
        return pltpu.VMEM(shape, jnp.bfloat16)

    def full_type(*shape):
        return pltpu.VMEM(shape, jnp.float32)

    return pl.pallas_call(
        mix_kernel,
        out_shape=pltpu.VMEM((rows // ways, model), jnp.bfloat16),
        in_specs=[pl.BlockSpec(memory_space=pl.ANY)] * len(big),
        out_specs=vmem,
        scratch_shapes=[pltpu.VMEM(array.shape, array.dtype) for array in big]
        + [
            half_type(mates, *tokens.shape),
            half_type(ways, rows, latent_down.shape[1]),
            half_type(ways, rows, query_down.shape[1]),
            half_type(EDGE, channels),
            half_type(EDGE, channels),
            full_type(EDGE + rows, channels),
            half_type(rows, channels),
            half_type(kvr, heads * NOPE),
            half_type(heads * VDIM, kvr),
            half_type(heads, 2 * NOPE + LANES, rows),
            half_type(blocks, ways, rows + ROPE, kvr // ways),
            half_type(2 * rows, heads * NOPE),
            half_type(heads, VDIM + ONES, 2 * rows),
            full_type(ring, 2 * rows, rows),
            half_type(ring, 2 * rows, rows),
            full_type(heads, 1, rows),
            full_type(heads, VDIM + ONES, rows),
            half_type(rows, heads * VDIM),
            full_type(rows, latent_down.shape[1] + query_down.shape[1] + LANES),
            full_type(rows, channels),
            full_type(rows, model),
            half_type(mates, rows // ways, model),
            half_type(mates, rows // ways, model),
            dma((len(big),)),
            dma((4, mates)),
            dma((4, mates)),
            dma((blocks // 4, 3)),
            dma((blocks // 4, 3)),
            dma((blocks,)),
            dma((blocks, mates)),
            dma((blocks, mates)),
            dma((mates, CHUNKS)),
            dma((mates, CHUNKS)),
        ],
        compiler_params=pltpu.CompilerParams(
            vmem_limit_bytes=60 * 1024 * 1024, collective_id=0, has_side_effects=True
        ),
    )(*big)


def solution(mesh):
    split = P(None, "tp")
    in_specs = (P("sp", "tp"),) + (split,) * 6 + (P(),) * 3 + (split,) * 2 + (P("tp", None),) * 2
    out_specs = P(("sp", "tp"), None)
    return jax.shard_map(local, mesh=mesh, in_specs=in_specs, out_specs=out_specs, check_vma=False)
```

```python
import jax
import numpy as np
import jax.numpy as jnp
from jax import lax
from jax.experimental import pallas as pl
from jax.experimental.pallas import tpu as pltpu
from jax.sharding import PartitionSpec as P

NOPE = 64
ROPE = 32
VDIM = 64
LANES = 128
ONES = 16
EDGE = 16
RING = 8
LAG = 2
EAGER = 9
CHUNKS = 2

MESH = pl.DeviceIdType.MESH
neg_fill = -1e30
rotary_base = 10000.0
norm_epsilon = 1e-06
log2e = 1.4426950408889634


def dot(a, b, dims=((1,), (0,))):
    return lax.dot_general(a, b, (dims, ((), ())), preferred_element_type=jnp.float32)


def unit(lat_parts, rot_parts, qx_ref, wk_ref, wvt_ref, keys, turned, scores, weights, best_ref, acc_ref, masked, low, heads):
    latent = jnp.concatenate(lat_parts, 0)
    rot = jnp.concatenate(rot_parts, 0)
    span = latent.shape[0]
    lanes = slice(low * NOPE, (low + heads) * NOPE)
    keys[:span, lanes] = dot(latent, wk_ref[:, lanes]).astype(jnp.bfloat16)
    flat = dot(wvt_ref[low * VDIM : (low + heads) * VDIM], latent, ((1,), (1,))).astype(jnp.bfloat16)
    for h in range(heads):
        turned[low + h, :VDIM, :span] = flat[h * VDIM : (h + 1) * VDIM]
    ring = scores.shape[0]
    tops = {}

    def score(h):
        pair = h // 2 * 2 * NOPE
        key = jnp.concatenate([keys[:span, pair : pair + 2 * NOPE], rot], 1)
        s = dot(key, qx_ref[h])
        if masked:
            k_at = lax.broadcasted_iota(jnp.int32, s.shape, 0)
            q_at = lax.broadcasted_iota(jnp.int32, s.shape, 1)
            s = jnp.where(k_at <= q_at, s, neg_fill)
        scores[h % ring, :span] = s
        top = jnp.max(s, 0, keepdims=True)
        if masked:
            tops[h] = (top, None)
        else:
            old = best_ref[h]
            top = jnp.maximum(old, top)
            tops[h] = (top, jnp.exp2(old - top))
        best_ref[h] = top

    def soften(h):
        weights[h % ring, :span] = jnp.exp2((scores[h % ring, :span] - tops[h][0]).astype(jnp.bfloat16))

    def gather(h):
        fresh = dot(turned[h, :, :span], weights[h % ring, :span])
        acc_ref[h] = fresh if masked else acc_ref[h] * tops[h][1] + fresh

    for step in range(heads + 2 * LAG):
        if step < heads:
            score(low + step)
        if 0 <= step - LAG < heads:
            soften(low + step - LAG)
        if 0 <= step - 2 * LAG < heads:
            gather(low + step - 2 * LAG)


def mix_kernel(
    inv_in, tok_in, ldown_in, rdown_in, qdown_in, up_in, inner_in, signal_in, lgain_in, qgain_in, qup_in, taps_in, outer_in, cproj_in, aproj_in,
    out_ref,
    inv_ref, tok, ldown, rdown, qdown, up_ref, inner_w, signal_w, lgain_ref, qgain_ref, qup, taps_ref, outer_w, cproj_ref, aproj_ref,
    xbuf, raw_lat, raw_query, edge, rim, padded, conv_ref, wk_ref, wvt_ref, qx_ref,
    kv, keys, turned, scores, weights, best_ref, acc_ref, att, small, held, cpart, part_buf, in_buf, far_query, far_qx, far_best, far_acc, back, back_top,
    load_sem, front_send, front_recv, up_send, side_send, kv_recv, share_send, share_recv, tail_send, tail_recv, far_sem, back_send, back_recv,
):
    me = lax.axis_index("sp")
    t = lax.axis_index("tp")
    total = lax.axis_size("sp")
    ways = lax.axis_size("tp")
    planes = total // 4
    z = me // 4
    b0 = me % 2
    b1 = (me // 2) % 2
    heads, _, rows = qx_ref.shape
    short = rows // ways
    span = 4 * (planes - 1)
    helper = z == 0
    helped = z == planes - 1
    deep = lax.select(helped, z - 1, z)
    cross = (1 - 2 * b0, 2 - 4 * b1, 3 - 2 * b0 - 4 * b1)
    after = lax.rem(me + 1, total)
    before = lax.rem(me + total - 1, total)
    mates = [lax.rem(t + o, ways) for o in range(1, ways)]

    barrier = pltpu.get_barrier_semaphore()
    targets = [(me, mate) for mate in mates] + [(me + c, t) for c in cross]
    targets += [(lax.rem(me + 4 * d, total), t) for d in range(1, planes)] + [(after, t), (before, t)]
    for target in targets:
        pl.semaphore_signal(barrier, inc=1, device_id=target, device_id_type=MESH)

    pairs = (
        (tok_in, tok), (ldown_in, ldown), (rdown_in, rdown), (qdown_in, qdown), (inv_in, inv_ref),
        (lgain_in, lgain_ref), (qgain_in, qgain_ref), (taps_in, taps_ref), (inner_in, inner_w), (up_in, up_ref),
        (qup_in, qup), (signal_in, signal_w), (outer_in, outer_w), (cproj_in, cproj_ref), (aproj_in, aproj_ref),
    )
    loads = [pltpu.make_async_copy(a, b, load_sem.at[i]) for i, (a, b) in enumerate(pairs)]
    for copy in loads[:EAGER]:
        copy.start()

    pl.semaphore_wait(barrier, len(targets))
    loads[0].wait()

    def to_mates(source, slots, kind):
        return [
            pltpu.make_async_remote_copy(
                source, slots.at[o], front_send.at[kind, o], front_recv.at[kind, o],
                device_id=(me, mate), device_id_type=MESH,
            )
            for o, mate in enumerate(mates)
        ]

    token_sends = to_mates(tok, xbuf, 0)
    for copy in token_sends:
        copy.start()
    loads[4].wait()
    half = ROPE // 2

    def turner(rank):
        position = (rank * rows + lax.broadcasted_iota(jnp.int32, (1, rows), 1)).astype(jnp.float32)
        angle = inv_ref[...] * position
        cosine = jnp.cos(angle)
        sine = jnp.sin(angle)

        def rotated(values):
            a = values[:half]
            b = values[half:]
            return jnp.concatenate([a * cosine - b * sine, a * sine + b * cosine], 0).astype(jnp.bfloat16)

        return rotated

    rotated = turner(me)
    for h in range(heads):
        turned[h, VDIM:] = jnp.ones((ONES, turned.shape[2]), jnp.bfloat16)
    depth = tok.shape[1]

    def rows_from(weight, o):
        at = pl.multiple_of(lax.rem(t + ways - o, ways) * depth, depth)
        if weight is rdown:
            return weight[:, pl.ds(at, depth)]
        return weight[pl.ds(at, depth), :]

    def project(x, weight, o):
        return dot(x, rows_from(weight, o), ((1,), (1 if weight is rdown else 0,)))

    def rest(value, weight):
        more = project(xbuf[0], weight, 1)
        for o in range(2, ways):
            more = more + project(xbuf[o - 1], weight, o)
        return value + more

    for copy in loads[1:4]:
        copy.wait()
    for copy in loads[EAGER:]:
        copy.start()
    narrow = (ldown, qdown, rdown)
    spots = []
    for weight in narrow:
        start = spots[-1].stop if spots else 0
        spots.append(slice(start, start + (LANES if weight is rdown else weight.shape[1])))
    for weight, spot in zip(narrow, spots):
        small[:, spot.start : spot.start + (ROPE if weight is rdown else weight.shape[1])] = project(tok[...], weight, 0)
    for copy in token_sends:
        copy.wait_recv()
    raw_lat[ways - 1] = rest(small[:, spots[0]], ldown).astype(jnp.bfloat16)
    latent_sends = to_mates(raw_lat.at[ways - 1], raw_lat, 1)
    query_sends = to_mates(raw_query.at[ways - 1], raw_query, 2)
    for copy in latent_sends:
        copy.start()
    raw_query[ways - 1] = rest(small[:, spots[1]], qdown).astype(jnp.bfloat16)
    for copy in query_sends:
        copy.start()
    ask = pltpu.make_async_remote_copy(
        raw_query.at[ways - 1], far_query.at[ways - 1], far_sem.at[0], far_sem.at[1],
        device_id=(lax.rem(me + 4, total), t), device_id_type=MESH,
    )

    @pl.when(helped)
    def _():
        ask.start()

    turn_part = rest(small[:, spots[2].start : spots[2].start + ROPE], rdown)
    turn = jnp.concatenate([turn_part, jnp.zeros((rows, LANES - ROPE), jnp.float32)], 1).T
    spun = rotated(turn[:ROPE])


    def whole(raw, gain_ref):
        values = jnp.concatenate([raw[lax.rem(t + ways - 1 - s, ways)] for s in range(ways)], 1).astype(jnp.float32)
        factor = lax.rsqrt(jnp.mean(values * values, -1, keepdims=True) + norm_epsilon)
        return (values * factor * gain_ref[...]).astype(jnp.bfloat16)

    for copy in latent_sends:
        copy.wait_recv()
    loads[5].wait()
    latent_norm = whole(raw_lat, lgain_ref)
    wide = kv.shape[3]
    for s in range(ways):
        kv[me, s, :rows] = latent_norm[:, s * wide : (s + 1) * wide]
        kv[me, s, rows:] = spun[:, s * wide : (s + 1) * wide]

    def send(j, target, sem):
        return pltpu.make_async_remote_copy(
            kv.at[j, t], kv.at[j, t], sem, kv_recv.at[j], device_id=(target, t), device_id_type=MESH
        )

    def shares(j):
        return [
            pltpu.make_async_remote_copy(
                kv.at[j, t], kv.at[j, t], share_send.at[j, o], share_recv.at[j, o],
                device_id=(me, mate), device_id_type=MESH,
            )
            for o, mate in enumerate(mates)
        ]

    def landed(j):
        for o in range(len(mates)):
            source = lax.rem(t + ways - 1 - o, ways)
            pltpu.make_async_remote_copy(
                kv.at[j, source], kv.at[j, source], share_send.at[j, o], share_recv.at[j, o],
                device_id=(me, mates[o]), device_id_type=MESH,
            ).wait_recv()

    def arrive(j):
        send(j, me, side_send.at[0, 0]).wait_recv()

    def collect(j):
        arrive(j)
        for copy in shares(j):
            copy.start()

    def lift(d, go, steps):
        for step in steps:
            starts = d % 4 == 0 if step > 1 else jnp.logical_or(d % 4 == 0, d % 4 == 3)

            @pl.when(jnp.logical_and(starts, z + step < planes - (z == d).astype(jnp.int32)))
            def _():
                go(send(me - 4 * d, me + 4 * step, up_send.at[d, step - 1]))

    def pass_on(d, ks):
        for k in ks:
            send(me - 4 * d, me + cross[k], side_send.at[d, k]).start()

    def relay(d, ks=(0, 1, 2)):
        j = me - 4 * d
        arrive(j)
        lift(d, begin, (1, 2, 3))
        pass_on(d, ks)
        for copy in shares(j):
            copy.start()

    def begin(copy):
        copy.start()

    def finish(copy):
        copy.wait_send()

    def own_side(go, ks):
        for k in ks:

            @pl.when(jnp.logical_or((b0, b1, b1)[k] == 0, helper))
            def _():
                go(send(me, me + cross[k], side_send.at[0, k]))

    lift(0, begin, (1,))
    own_side(begin, (0, 1))
    loads[9].wait()
    low = lax.broadcasted_iota(jnp.int32, (1, 2 * NOPE), 1) < NOPE
    width = NOPE + VDIM
    for p in range(heads // 2):
        even = up_ref[:, 2 * p * width : (2 * p + 1) * width].astype(jnp.float32)
        odd = up_ref[:, (2 * p + 1) * width : (2 * p + 2) * width].astype(jnp.float32)
        at = slice(p * width, (p + 1) * width)
        wk_ref[:, at] = jnp.where(low, even, pltpu.roll(odd, NOPE, 1)).astype(jnp.bfloat16)
        wvt_ref[at] = jnp.where(low, pltpu.roll(even, NOPE, 1), odd).T.astype(jnp.bfloat16)

    loads[6].wait()
    loads[10].wait()
    for copy in query_sends:
        copy.wait_recv()
    def prepare(raw, spin, queries):
        scale = (NOPE + ROPE) ** (-0.5) * log2e
        query = (dot(whole(raw, qgain_ref), qup[...]) * scale).T
        size = NOPE + ROPE
        for h in range(heads):
            base = h * size
            side = h % 2 * NOPE
            queries[h, side : side + NOPE] = query[base : base + NOPE].astype(jnp.bfloat16)
            queries[h, NOPE - side : 2 * NOPE - side] = jnp.zeros((NOPE, rows), jnp.bfloat16)
            queries[h, 2 * NOPE : 2 * NOPE + ROPE] = spin(query[base + NOPE : base + size])
            queries[h, 2 * NOPE + ROPE :] = jnp.zeros((LANES - ROPE, rows), jnp.bfloat16)

    prepare(raw_query, rotated, qx_ref)

    def run(blocks, masked, queries=qx_ref, best=best_ref, acc=acc_ref, low=0, count=heads):
        lat_parts = []
        rot_parts = []
        for j in blocks:
            lat_parts.append(jnp.concatenate([kv[j, s, :rows] for s in range(ways)], 1))
            spin = jnp.concatenate([kv[j, s, rows:] for s in range(ways)], 1).astype(jnp.float32)
            spin = jnp.concatenate([spin, jnp.zeros((LANES - ROPE, rows), jnp.float32)], 0)
            rot_parts.append(spin.T.astype(jnp.bfloat16))
        unit(
            lat_parts, rot_parts, queries, wk_ref, wvt_ref, keys, turned, scores, weights, best, acc, masked, low, count
        )

    lift(0, begin, (2,))
    own_side(begin, (2,))
    run([me], True)
    lift(0, begin, (3,))
    loads[8].wait()
    inner = rest(project(tok[...], inner_w, 0), inner_w)
    loads[11].wait()
    signal = rest(project(tok[...], signal_w, 0), signal_w)
    gated = (inner * signal).astype(jnp.bfloat16)
    padded[EDGE:] = gated.astype(jnp.float32)
    edge[...] = gated[rows - EDGE :]
    rim_copy = pltpu.make_async_remote_copy(
        edge, rim, front_send.at[3, 0], front_recv.at[3, 0], device_id=(after, t), device_id_type=MESH
    )

    @pl.when(me + 1 < total)
    def _():
        rim_copy.start()

    @pl.when(deep > 0)
    def _():
        relay(1, (0, 1))

    loads[12].wait()
    held[...] = rest(project(tok[...], outer_w, 0), outer_w)

    @pl.when(deep > 0)
    def _():
        pass_on(1, (2,))


    far_shares = to_mates(far_query.at[ways - 1], far_query, 4)
    groups, members = back_top.shape[:2]

    def returns(g):
        return [
            pltpu.make_async_remote_copy(
                buf.at[g], buf.at[g], back_send.at[g, i], back_recv.at[g, i],
                device_id=(lax.rem(me + span, total), t), device_id_type=MESH,
            )
            for i, buf in enumerate((back, back_top))
        ]

    @pl.when(helper)
    def _():
        ask.wait_recv()
        for copy in far_shares:
            copy.start()
        for c in cross:
            collect(me + c)
        for copy in far_shares:
            copy.wait_recv()
        prepare(far_query, turner(me + span), far_qx)
        far_best[...] = jnp.full(far_best.shape, neg_fill, jnp.float32)
        far_acc[...] = jnp.zeros(far_acc.shape, jnp.float32)
        base = me - me % 4
        for c in cross:
            landed(me + c)
        for g in range(groups):

            @pl.loop(0, 2)
            def _(p):
                run([base + 2 * p, base + 2 * p + 1], False, far_qx, far_best, far_acc, g * members, members)

            for i in range(members):
                acc = far_acc[g * members + i]
                mass = acc[VDIM : VDIM + 1]
                back[g, i] = (acc[:VDIM] * (1.0 / mass)).astype(jnp.bfloat16)
                back_top[g, i : i + 1] = far_best[g * members + i] + jnp.log2(mass)
            for copy in returns(g):
                copy.start()

    lower = jnp.logical_not(helper)

    @pl.when(jnp.logical_and(b0 == 1, lower))
    def _():
        collect(me + cross[0])
        landed(me + cross[0])

    @pl.when(b0 == 1)
    def _():
        run([me + cross[0]], False)

    @pl.when(jnp.logical_and(b1 == 1, lower))
    def _():
        collect(me + cross[1])
        collect(me + cross[2])

    def convolve():
        loads[7].wait()

        @pl.when(me > 0)
        def _():
            rim_copy.wait_recv()
            padded[:EDGE] = rim[...].astype(jnp.float32)

        @pl.when(me == 0)
        def _():
            padded[:EDGE] = jnp.zeros((EDGE, padded.shape[1]), jnp.float32)

        reach = taps_ref.shape[0] - 1
        taps = taps_ref[...].astype(jnp.float32)
        filtered = padded[EDGE:] * taps[reach : reach + 1, :]
        for k in range(reach):
            filtered = filtered + padded[EDGE - reach + k : EDGE - reach + k + rows] * taps[k : k + 1, :]
        conv_ref[...] = (held[...] * filtered).astype(jnp.bfloat16)

        loads[13].wait()
        cpart[...] = dot(conv_ref[...], cproj_ref[...])

    @pl.loop(0, 2 * deep + 1)
    def _(n):
        plane = (n + 1) // 2
        odd = n % 2
        own = me - 4 * plane

        def ahead(when):
            then = me - 4 * ((n + 2) // 2)

            @pl.when(jnp.logical_and(when, jnp.logical_and(n < 2 * deep, odd == 0)))
            def _():
                collect(then + cross[0])

            @pl.when(jnp.logical_and(when, jnp.logical_and(n < 2 * deep, odd == 1)))
            def _():
                collect(then + cross[1])
                collect(then + cross[2])

        @pl.when(jnp.logical_and(n == 0, b1 == 1))
        def _():
            convolve()

        late = jnp.logical_and(n == 1, b1 == 0)
        ahead(jnp.logical_not(late))
        far = (n + b1) // 2 + 2

        @pl.when(jnp.logical_and(jnp.logical_or(n == 0, (n + b1) % 2 == 0), far <= deep))
        def _():
            relay(far)

        @pl.when(jnp.logical_and(n == 0, b1 == 0))
        def _():
            convolve()

        left = own + (1 - odd) * cross[1]
        right = own + odd * cross[0] + (1 - odd) * cross[2]

        @pl.when(jnp.logical_and(n + b1 > 0, lower))
        def _():
            landed(left)
            landed(right)

        @pl.when(n + b1 > 0)
        def _():
            run([left, right], False)

        ahead(late)

    @pl.when(helped)
    def _():
        for g in range(groups):
            for copy in returns(g):
                copy.wait_recv()
            for i in range(members):
                h = g * members + i
                mine = best_ref[h]
                other = back_top[g, i : i + 1]
                top = jnp.maximum(mine, other)
                keep = jnp.exp2(mine - top)
                add = jnp.exp2(other - top)
                acc_ref[h, :VDIM] = acc_ref[h, :VDIM] * keep + back[g, i].astype(jnp.float32) * add
                acc_ref[h, VDIM:] = acc_ref[h, VDIM:] * keep + add

    loads[14].wait()

    def settle(at):
        flat = []
        for h in range(heads):
            acc = acc_ref[h, :, at]
            flat.append(acc[:VDIM] * (1.0 / acc[VDIM : VDIM + 1]))
        return jnp.concatenate(flat, 0).T.astype(jnp.bfloat16)

    if short % LANES:
        att[...] = settle(slice(None))

    model = cpart.shape[1]
    step = model // CHUNKS

    def rows_of(owner):
        at = pl.ds(pl.multiple_of(owner * short, short), short)
        return at, (att[at, :] if short % LANES else settle(at))

    def part(at, mixed, c):
        cols = slice(c * step, (c + 1) * step)
        return (cpart[at, cols] + dot(mixed, aproj_ref[:, cols])).astype(jnp.bfloat16)

    tails = []
    for o, mate in enumerate(mates):
        at, mixed = rows_of(mate)
        for c in range(CHUNKS):
            cols = pl.ds(c * step, step)
            part_buf[o, :, cols] = part(at, mixed, c)
            tails.append(
                pltpu.make_async_remote_copy(
                    part_buf.at[o, :, cols], in_buf.at[o, :, cols], tail_send.at[o, c], tail_recv.at[o, c],
                    device_id=(me, mate), device_id_type=MESH,
                )
            )
            tails[-1].start()
    at, mixed = rows_of(t)
    for c in range(CHUNKS):
        cpart[:short, c * step : (c + 1) * step] = part(at, mixed, c).astype(jnp.float32)
    for c in range(CHUNKS):
        cols = slice(c * step, (c + 1) * step)
        result = cpart[:short, cols]
        for o in range(len(mates)):
            tails[o * CHUNKS + c].wait_recv()
            result = result + in_buf[o, :, cols].astype(jnp.float32)
        out_ref[:, cols] = result.astype(jnp.bfloat16)
    for copy in tails + token_sends + latent_sends + query_sends:
        copy.wait_send()

    @pl.when(me + 1 < total)
    def _():
        rim_copy.wait_send()

    lift(0, finish, (1, 2, 3))
    own_side(finish, (0, 1, 2))

    @pl.when(helped)
    def _():
        ask.wait_send()

    @pl.when(helper)
    def _():
        for copy in far_shares:
            copy.wait_send()
        for g in range(groups):
            for copy in returns(g):
                copy.wait_send()

    @pl.when(jnp.logical_or(b0 == 1, helper))
    def _():
        for copy in shares(me + cross[0]):
            copy.wait_send()

    @pl.when(jnp.logical_or(b1 == 1, helper))
    def _():
        for copy in shares(me + cross[1]) + shares(me + cross[2]):
            copy.wait_send()

    @pl.loop(1, deep + 1)
    def _(d):
        j = me - 4 * d
        lift(d, finish, (1, 2, 3))
        for k in range(3):
            send(j, me + cross[k], side_send.at[d, k]).wait_send()
        for c in (0,) + cross:
            for copy in shares(j + c):
                copy.wait_send()


def local(
    tokens,
    outer_gate,
    inner_gate,
    conv_input,
    conv_taps,
    query_down,
    latent_down,
    rotary_down,
    query_gain,
    latent_gain,
    query_up,
    latent_up,
    conv_project,
    attend_project,
):
    rows = tokens.shape[0]
    heads = query_up.shape[1] // (NOPE + ROPE)
    ways = lax.axis_size("tp")
    blocks = lax.axis_size("sp")
    model = conv_project.shape[1]
    kvr = latent_up.shape[0]
    channels = conv_project.shape[0]
    half = ROPE // 2
    inverse = jnp.asarray(np.float32(rotary_base) ** (-(np.arange(half, dtype=np.float32) * 2.0 / (2 * half))), jnp.float32)
    vmem = pl.BlockSpec(memory_space=pltpu.VMEM)
    dma = pltpu.SemaphoreType.DMA
    mates = ways - 1
    ring = min(heads, RING)
    groups = 1 if heads % 4 else 2
    big = (
        inverse[:, None], tokens, latent_down, rotary_down.T, query_down, latent_up, inner_gate, conv_input,
        latent_gain[None, :], query_gain[None, :], query_up, conv_taps, outer_gate, conv_project, attend_project,
    )

    def half_type(*shape):
        return pltpu.VMEM(shape, jnp.bfloat16)

    def full_type(*shape):
        return pltpu.VMEM(shape, jnp.float32)

    return pl.pallas_call(
        mix_kernel,
        out_shape=pltpu.VMEM((rows // ways, model), jnp.bfloat16),
        in_specs=[pl.BlockSpec(memory_space=pl.ANY)] * len(big),
        out_specs=vmem,
        scratch_shapes=[pltpu.VMEM(array.shape, array.dtype) for array in big]
        + [
            half_type(mates, *tokens.shape),
            half_type(ways, rows, latent_down.shape[1]),
            half_type(ways, rows, query_down.shape[1]),
            half_type(EDGE, channels),
            half_type(EDGE, channels),
            full_type(EDGE + rows, channels),
            half_type(rows, channels),
            half_type(kvr, heads * NOPE),
            half_type(heads * VDIM, kvr),
            half_type(heads, 2 * NOPE + LANES, rows),
            half_type(blocks, ways, rows + ROPE, kvr // ways),
            half_type(2 * rows, heads * NOPE),
            half_type(heads, VDIM + ONES, 2 * rows),
            full_type(ring, 2 * rows, rows),
            half_type(ring, 2 * rows, rows),
            full_type(heads, 1, rows),
            full_type(heads, VDIM + ONES, rows),
            half_type(rows, heads * VDIM),
            full_type(rows, latent_down.shape[1] + query_down.shape[1] + LANES),
            full_type(rows, channels),
            full_type(rows, model),
            half_type(mates, rows // ways, model),
            half_type(mates, rows // ways, model),
            half_type(ways, rows, query_down.shape[1]),
            half_type(heads, 2 * NOPE + LANES, rows),
            full_type(heads, 1, rows),
            full_type(heads, VDIM + ONES, rows),
            half_type(groups, heads // groups, VDIM, rows),
            full_type(groups, heads // groups, rows),
            dma((len(big),)),
            dma((5, mates)),
            dma((5, mates)),
            dma((blocks // 4, 3)),
            dma((blocks // 4, 3)),
            dma((blocks,)),
            dma((blocks, mates)),
            dma((blocks, mates)),
            dma((mates, CHUNKS)),
            dma((mates, CHUNKS)),
            dma((2,)),
            dma((groups, 2)),
            dma((groups, 2)),
        ],
        compiler_params=pltpu.CompilerParams(
            vmem_limit_bytes=60 * 1024 * 1024, collective_id=0, has_side_effects=True
        ),
    )(*big)


def solution(mesh):
    split = P(None, "tp")
    in_specs = (P("sp", "tp"),) + (split,) * 6 + (P(),) * 3 + (split,) * 2 + (P("tp", None),) * 2
    out_specs = P(("sp", "tp"), None)
    return jax.shard_map(local, mesh=mesh, in_specs=in_specs, out_specs=out_specs, check_vma=False)
```

```python
import jax
import numpy as np
import jax.numpy as jnp
from jax import lax
from jax.experimental import pallas as pl
from jax.experimental.pallas import tpu as pltpu
from jax.sharding import PartitionSpec as P

NOPE = 64
ROPE = 32
VDIM = 64
LANES = 128
ONES = 16
EDGE = 16
RING = 8
LAG = 2
EAGER = 9
CHUNKS = 2
TAG = 16

MESH = pl.DeviceIdType.MESH
neg_fill = -1e30
rotary_base = 10000.0
norm_epsilon = 1e-06
log2e = 1.4426950408889634


def dot(a, b, dims=((1,), (0,))):
    return lax.dot_general(a, b, (dims, ((), ())), preferred_element_type=jnp.float32)


def unit(lat_parts, rot_parts, factors, qx_ref, wk_ref, wvt_ref, keys, turned, scores, weights, best_ref, acc_ref, masked, low, heads):
    latent = jnp.concatenate(lat_parts, 0)
    rot = jnp.concatenate(rot_parts, 0)
    span = latent.shape[0]
    lanes = slice(low * NOPE, (low + heads) * NOPE)
    down = jnp.concatenate([f[0] for f in factors], 0)
    along = jnp.concatenate([f[1] for f in factors], 1)
    keys[:span, lanes] = (dot(latent, wk_ref[:, lanes]) * down).astype(jnp.bfloat16)
    flat = dot(wvt_ref[low * VDIM : (low + heads) * VDIM], latent, ((1,), (1,)))
    flat = (flat * along).astype(jnp.bfloat16)
    for h in range(heads):
        turned[low + h, :VDIM, :span] = flat[h * VDIM : (h + 1) * VDIM]
    ring = scores.shape[0]
    tops = {}

    def score(h):
        pair = h // 2 * 2 * NOPE
        key = jnp.concatenate([keys[:span, pair : pair + 2 * NOPE], rot], 1)
        s = dot(key, qx_ref[h])
        if masked:
            k_at = lax.broadcasted_iota(jnp.int32, s.shape, 0)
            q_at = lax.broadcasted_iota(jnp.int32, s.shape, 1)
            s = jnp.where(k_at <= q_at, s, neg_fill)
        scores[h % ring, :span] = s
        top = jnp.max(s, 0, keepdims=True)
        if masked:
            tops[h] = (top, None)
        else:
            old = best_ref[h]
            top = jnp.maximum(old, top)
            tops[h] = (top, jnp.exp2(old - top))
        best_ref[h] = top

    def soften(h):
        weights[h % ring, :span] = jnp.exp2((scores[h % ring, :span] - tops[h][0]).astype(jnp.bfloat16))

    def gather(h):
        fresh = dot(turned[h, :, :span], weights[h % ring, :span])
        acc_ref[h] = fresh if masked else acc_ref[h] * tops[h][1] + fresh

    for step in range(heads + 2 * LAG):
        if step < heads:
            score(low + step)
        if 0 <= step - LAG < heads:
            soften(low + step - LAG)
        if 0 <= step - 2 * LAG < heads:
            gather(low + step - 2 * LAG)


def mix_kernel(
    inv_in, tok_in, ldown_in, rdown_in, qdown_in, up_in, inner_in, signal_in, lgain_in, qgain_in, qup_in, taps_in, outer_in, cproj_in, aproj_in,
    out_ref,
    inv_ref, tok, ldown, rdown, qdown, up_ref, inner_w, signal_w, lgain_ref, qgain_ref, qup, taps_ref, outer_w, cproj_ref, aproj_ref,
    xbuf, comb, raw_query, edge, rim, padded, conv_ref, wk_ref, wvt_ref, qx_ref,
    kv, keys, turned, scores, weights, best_ref, acc_ref, att, small, held, cpart, part_buf, in_buf, far_query, far_qx, far_best, far_acc, back, back_top,
    load_sem, front_send, front_recv, up_send, side_send, kv_recv, share_send, share_recv, tail_send, tail_recv, far_sem, back_send, back_recv,
):
    me = lax.axis_index("sp")
    t = lax.axis_index("tp")
    total = lax.axis_size("sp")
    ways = lax.axis_size("tp")
    planes = total // 4
    z = me // 4
    b0 = me % 2
    b1 = (me // 2) % 2
    heads, _, rows = qx_ref.shape
    short = rows // ways
    span = 4 * (planes - 1)
    helper = z == 0
    helped = z == planes - 1
    deep = lax.select(helped, z - 1, z)
    cross = (1 - 2 * b0, 2 - 4 * b1, 3 - 2 * b0 - 4 * b1)
    after = lax.rem(me + 1, total)
    before = lax.rem(me + total - 1, total)
    mates = [lax.rem(t + o, ways) for o in range(1, ways)]

    barrier = pltpu.get_barrier_semaphore()
    targets = [(me, mate) for mate in mates] + [(me + c, t) for c in cross]
    targets += [(lax.rem(me + 4 * d, total), t) for d in range(1, planes)]
    for target in targets:
        pl.semaphore_signal(barrier, inc=1, device_id=target, device_id_type=MESH)

    @pl.when(me > 0)
    def _():
        pl.semaphore_signal(barrier, inc=1, device_id=(before, t), device_id_type=MESH)

    @pl.when(me + 1 < total)
    def _():
        pl.semaphore_signal(barrier, inc=1, device_id=(after, t), device_id_type=MESH)

    ends = (me == 0).astype(jnp.int32) + (me + 1 == total).astype(jnp.int32)

    pairs = (
        (tok_in, tok), (ldown_in, ldown), (rdown_in, rdown), (qdown_in, qdown), (inv_in, inv_ref),
        (lgain_in, lgain_ref), (qgain_in, qgain_ref), (taps_in, taps_ref), (inner_in, inner_w), (up_in, up_ref),
        (qup_in, qup), (signal_in, signal_w), (outer_in, outer_w), (cproj_in, cproj_ref), (aproj_in, aproj_ref),
    )
    loads = [pltpu.make_async_copy(a, b, load_sem.at[i]) for i, (a, b) in enumerate(pairs)]
    for copy in loads[:EAGER]:
        copy.start()

    pl.semaphore_wait(barrier, len(targets) + 2 - ends)
    loads[0].wait()

    def to_mates(source, slots, kind):
        return [
            pltpu.make_async_remote_copy(
                source, slots.at[o], front_send.at[kind, o], front_recv.at[kind, o],
                device_id=(me, mate), device_id_type=MESH,
            )
            for o, mate in enumerate(mates)
        ]

    token_sends = to_mates(tok, xbuf, 0)
    for copy in token_sends:
        copy.start()
    loads[4].wait()
    half = ROPE // 2

    def turner(rank):
        position = (rank * rows + lax.broadcasted_iota(jnp.int32, (1, rows), 1)).astype(jnp.float32)
        angle = inv_ref[...] * position
        cosine = jnp.cos(angle)
        sine = jnp.sin(angle)

        def rotated(values):
            a = values[:half]
            b = values[half:]
            return jnp.concatenate([a * cosine - b * sine, a * sine + b * cosine], 0).astype(jnp.bfloat16)

        return rotated

    rotated = turner(me)
    for h in range(heads):
        turned[h, VDIM:] = jnp.ones((ONES, turned.shape[2]), jnp.bfloat16)
    depth = tok.shape[1]

    def rows_from(weight, o):
        at = pl.multiple_of(lax.rem(t + ways - o, ways) * depth, depth)
        return weight[pl.ds(at, depth), :]

    def project(x, weight, o):
        return dot(x, rows_from(weight, o))

    def rest(value, weight):
        more = project(xbuf[0], weight, 1)
        for o in range(2, ways):
            more = more + project(xbuf[o - 1], weight, o)
        return value + more

    for copy in loads[1:4]:
        copy.wait()
    for copy in loads[EAGER:]:
        copy.start()
    wide = kv.shape[3]
    if wide < LANES:
        comb[:, :LANES] = jnp.zeros((comb.shape[0], LANES), jnp.bfloat16)
    comb[:, :wide] = ldown[...]
    tall = jnp.concatenate([rdown[...].astype(jnp.float32), jnp.zeros((LANES - ROPE, comb.shape[0]), jnp.float32)], 0)
    comb[:, LANES:] = tall.T.astype(jnp.bfloat16)
    small[:, : 2 * LANES] = project(tok[...], comb, 0)
    small[:, 2 * LANES :] = project(tok[...], qdown, 0)
    for copy in token_sends:
        copy.wait_recv()
    both = rest(small[:, : 2 * LANES], comb)
    raw_query[ways - 1] = rest(small[:, 2 * LANES :], qdown).astype(jnp.bfloat16)
    piece = both[:, :wide].astype(jnp.bfloat16)
    kv[me, t, :rows] = piece
    mass = piece.astype(jnp.float32)
    mass = jnp.sum(mass * mass, -1, keepdims=True)
    lane = lax.broadcasted_iota(jnp.int32, (1, LANES), 1)
    turn = jnp.where(lane == ROPE, mass, both[:, LANES:]).T
    spun = rotated(turn[:ROPE])
    for s in range(ways):

        @pl.when(t == s)
        def _():
            kv[me, s, rows : rows + ROPE] = spun[:, s * wide : (s + 1) * wide]

    mass = turn[ROPE : ROPE + 1]
    high = mass.astype(jnp.bfloat16).astype(jnp.float32)
    folds = rows // wide
    tags = [part[:, r * wide : (r + 1) * wide] for part in (high, mass - high) for r in range(folds)]
    if len(tags) < TAG:
        tags.append(jnp.zeros((TAG - len(tags), wide), jnp.float32))
    kv[me, t, rows + ROPE :] = jnp.concatenate(tags, 0).astype(jnp.bfloat16)

    def whole(raw, gain_ref):
        values = jnp.concatenate([raw[lax.rem(t + ways - 1 - s, ways)] for s in range(ways)], 1).astype(jnp.float32)
        factor = lax.rsqrt(jnp.mean(values * values, -1, keepdims=True) + norm_epsilon)
        return (values * factor * gain_ref[...]).astype(jnp.bfloat16)

    def send(j, target, sem):
        return pltpu.make_async_remote_copy(
            kv.at[j, t], kv.at[j, t], sem, kv_recv.at[j], device_id=(target, t), device_id_type=MESH
        )

    def shares(j):
        return [
            pltpu.make_async_remote_copy(
                kv.at[j, t], kv.at[j, t], share_send.at[j, o], share_recv.at[j, o],
                device_id=(me, mate), device_id_type=MESH,
            )
            for o, mate in enumerate(mates)
        ]

    def landed(j):
        for o in range(len(mates)):
            source = lax.rem(t + ways - 1 - o, ways)
            pltpu.make_async_remote_copy(
                kv.at[j, source], kv.at[j, source], share_send.at[j, o], share_recv.at[j, o],
                device_id=(me, mates[o]), device_id_type=MESH,
            ).wait_recv()

    def arrive(j):
        send(j, me, side_send.at[0, 0]).wait_recv()

    def collect(j):
        arrive(j)
        for copy in shares(j):
            copy.start()

    def lift(d, go, steps):
        for step in steps:
            starts = d % 4 == 0 if step > 1 else jnp.logical_or(d % 4 == 0, d % 4 == 3)

            @pl.when(jnp.logical_and(starts, z + step < planes - (z == d).astype(jnp.int32)))
            def _():
                go(send(me - 4 * d, me + 4 * step, up_send.at[d, step - 1]))

    def pass_on(d, ks):
        for k in ks:
            send(me - 4 * d, me + cross[k], side_send.at[d, k]).start()

    def relay(d, ks=(0, 1, 2)):
        j = me - 4 * d
        arrive(j)
        lift(d, begin, (1, 2, 3))
        pass_on(d, ks)
        for copy in shares(j):
            copy.start()

    def begin(copy):
        copy.start()

    def finish(copy):
        copy.wait_send()

    def own_side(go, ks):
        for k in ks:

            @pl.when(jnp.logical_or((b0, b1, b1)[k] == 0, helper))
            def _():
                go(send(me, me + cross[k], side_send.at[0, k]))

    query_sends = to_mates(raw_query.at[ways - 1], raw_query, 2)
    for copy in query_sends:
        copy.start()
    ask = pltpu.make_async_remote_copy(
        raw_query.at[ways - 1], far_query.at[ways - 1], far_sem.at[0], far_sem.at[1],
        device_id=(lax.rem(me + 4, total), t), device_id_type=MESH,
    )

    @pl.when(helped)
    def _():
        ask.start()

    lift(0, begin, (1,))
    own_side(begin, (0, 1))
    for copy in shares(me):
        copy.start()
    loads[8].wait()
    inner = rest(project(tok[...], inner_w, 0), inner_w)
    loads[11].wait()
    signal = rest(project(tok[...], signal_w, 0), signal_w)
    gated = (inner * signal).astype(jnp.bfloat16)
    padded[EDGE:] = gated.astype(jnp.float32)
    edge[...] = gated[rows - EDGE :]
    rim_copy = pltpu.make_async_remote_copy(
        edge, rim, front_send.at[3, 0], front_recv.at[3, 0], device_id=(after, t), device_id_type=MESH
    )

    @pl.when(me + 1 < total)
    def _():
        rim_copy.start()

    loads[5].wait()
    loads[9].wait()
    low = lax.broadcasted_iota(jnp.int32, (1, 2 * NOPE), 1) < NOPE
    width = NOPE + VDIM
    gain = jnp.concatenate([lgain_ref[...], jnp.zeros((LANES - 1, lgain_ref.shape[1]), jnp.float32)], 0).T[:, :1]
    for p in range(heads // 2):
        even = up_ref[:, 2 * p * width : (2 * p + 1) * width].astype(jnp.float32) * gain
        odd = up_ref[:, (2 * p + 1) * width : (2 * p + 2) * width].astype(jnp.float32) * gain
        at = slice(p * width, (p + 1) * width)
        wk_ref[:, at] = jnp.where(low, even, pltpu.roll(odd, NOPE, 1)).astype(jnp.bfloat16)
        wvt_ref[at] = jnp.where(low, pltpu.roll(even, NOPE, 1), odd).T.astype(jnp.bfloat16)

    loads[6].wait()
    loads[10].wait()
    for copy in query_sends:
        copy.wait_recv()
    def prepare(raw, spin, queries):
        scale = (NOPE + ROPE) ** (-0.5) * log2e
        query = (dot(whole(raw, qgain_ref), qup[...]) * scale).T
        size = NOPE + ROPE
        for h in range(heads):
            base = h * size
            side = h % 2 * NOPE
            queries[h, side : side + NOPE] = query[base : base + NOPE].astype(jnp.bfloat16)
            queries[h, NOPE - side : 2 * NOPE - side] = jnp.zeros((NOPE, rows), jnp.bfloat16)
            queries[h, 2 * NOPE : 2 * NOPE + ROPE] = spin(query[base + NOPE : base + size])
            queries[h, 2 * NOPE + ROPE :] = jnp.zeros((LANES - ROPE, rows), jnp.bfloat16)

    prepare(raw_query, rotated, qx_ref)

    def run(blocks, masked, queries=qx_ref, best=best_ref, acc=acc_ref, low=0, count=heads):
        lat_parts = []
        rot_parts = []
        factors = []
        for j in blocks:
            lat_parts.append(jnp.concatenate([kv[j, s, :rows] for s in range(ways)], 1))
            spin = jnp.concatenate([kv[j, s, rows : rows + ROPE] for s in range(ways)], 1).astype(jnp.float32)
            tag = kv[j, 0, rows + ROPE :].astype(jnp.float32)
            for s in range(1, ways):
                tag = tag + kv[j, s, rows + ROPE :].astype(jnp.float32)
            mass = jnp.concatenate([tag[r : r + 1] + tag[folds + r : folds + r + 1] for r in range(folds)], 1)
            along = lax.rsqrt(mass * (1.0 / (ways * wide)) + norm_epsilon)
            spin = jnp.concatenate([spin, along, jnp.zeros((LANES - ROPE - 1, rows), jnp.float32)], 0).T
            rot_parts.append(spin.astype(jnp.bfloat16))
            factors.append((spin[:, ROPE : ROPE + 1], along))
        unit(
            lat_parts, rot_parts, factors, queries, wk_ref, wvt_ref, keys, turned, scores, weights, best, acc, masked, low, count
        )

    lift(0, begin, (2,))
    own_side(begin, (2,))
    loads[12].wait()
    held[...] = rest(project(tok[...], outer_w, 0), outer_w)

    @pl.when(deep > 0)
    def _():
        relay(1, (0, 1))


    landed(me)
    run([me], True)
    lift(0, begin, (3,))

    @pl.when(deep > 0)
    def _():
        pass_on(1, (2,))


    far_shares = to_mates(far_query.at[ways - 1], far_query, 4)
    groups = back_send.shape[0]
    bounds = [(g * heads // groups, heads // groups) for g in range(groups)]

    def returns(g):
        return [
            pltpu.make_async_remote_copy(
                buf.at[pl.ds(*bounds[g])], buf.at[pl.ds(*bounds[g])], back_send.at[g, i], back_recv.at[g, i],
                device_id=(lax.rem(me + span, total), t), device_id_type=MESH,
            )
            for i, buf in enumerate((back, back_top))
        ]

    @pl.when(helper)
    def _():
        ask.wait_recv()
        for copy in far_shares:
            copy.start()
        far_best[...] = jnp.full(far_best.shape, neg_fill, jnp.float32)
        far_acc[...] = jnp.zeros(far_acc.shape, jnp.float32)
        for c in cross:
            collect(me + c)
        for copy in far_shares:
            copy.wait_recv()
        prepare(far_query, turner(me + span), far_qx)
        landed(me + cross[0])
        for g in range(groups):

            @pl.loop(0, 2)
            def _(p):
                if g == 0:

                    @pl.when(p == 1)
                    def _():
                        landed(me + cross[1])
                        landed(me + cross[2])

                first = me + p * cross[1]
                then = me + (1 - p) * cross[0] + p * cross[2]
                run([first, then], False, far_qx, far_best, far_acc, *bounds[g])

            for h in range(bounds[g][0], sum(bounds[g])):
                acc = far_acc[h]
                mass = acc[VDIM : VDIM + 1]
                back[h] = (acc[:VDIM] * (1.0 / mass)).astype(jnp.bfloat16)
                back_top[h] = far_best[h] + jnp.log2(mass)
            for copy in returns(g):
                copy.start()

    lower = jnp.logical_not(helper)
    corner = jnp.logical_and(b0 + b1 == 0, deep > 0)

    @pl.when(jnp.logical_and(b0 == 1, lower))
    def _():
        collect(me + cross[0])
        landed(me + cross[0])

    alone = lax.select(corner, me - 4, me + cross[0])

    @pl.when(corner)
    def _():
        landed(alone)

    @pl.when(jnp.logical_or(b0 == 1, corner))
    def _():
        run([alone], False)

    @pl.when(jnp.logical_and(b1 == 1, lower))
    def _():
        collect(me + cross[1])
        collect(me + cross[2])

    def convolve():
        loads[7].wait()

        @pl.when(me > 0)
        def _():
            rim_copy.wait_recv()
            padded[:EDGE] = rim[...].astype(jnp.float32)

        @pl.when(me == 0)
        def _():
            padded[:EDGE] = jnp.zeros((EDGE, padded.shape[1]), jnp.float32)

        reach = taps_ref.shape[0] - 1
        taps = taps_ref[...].astype(jnp.float32)
        filtered = padded[EDGE:] * taps[reach : reach + 1, :]
        for k in range(reach):
            filtered = filtered + padded[EDGE - reach + k : EDGE - reach + k + rows] * taps[k : k + 1, :]
        conv_ref[...] = (held[...] * filtered).astype(jnp.bfloat16)

        loads[13].wait()
        cpart[...] = dot(conv_ref[...], cproj_ref[...])

    @pl.loop(0, 2 * deep + 1)
    def _(n):
        plane = (n + 1) // 2
        odd = n % 2
        own = me - 4 * plane

        def ahead(when):
            then = me - 4 * ((n + 2) // 2)

            @pl.when(jnp.logical_and(when, jnp.logical_and(n < 2 * deep, odd == 0)))
            def _():
                collect(then + cross[0])

            @pl.when(jnp.logical_and(when, jnp.logical_and(n < 2 * deep, jnp.logical_xor(odd == 1, corner))))
            def _():
                collect(then + cross[1])

            @pl.when(jnp.logical_and(when, jnp.logical_and(n < 2 * deep, odd == 1)))
            def _():
                collect(then + cross[2])

        @pl.when(jnp.logical_and(n == 0, b1 == 1))
        def _():
            convolve()

        late = jnp.logical_and(n == 1, b1 == 0)
        ahead(jnp.logical_not(late))
        far = (n + b1) // 2 + 2

        @pl.when(jnp.logical_and(jnp.logical_or(n == 0, (n + b1) % 2 == 0), far <= deep))
        def _():
            relay(far)

        @pl.when(jnp.logical_and(n == 0, b1 == 0))
        def _():
            convolve()

        left = lax.select(corner, own + odd * cross[0] + (1 - odd) * cross[2], own + (1 - odd) * cross[1])
        right = lax.select(
            corner, own + odd * cross[1] - (1 - odd) * 4, own + odd * cross[0] + (1 - odd) * cross[2]
        )
        full = jnp.logical_and(n + b1 > 0, jnp.logical_not(jnp.logical_and(corner, n == 2 * deep)))

        @pl.when(jnp.logical_and(full, lower))
        def _():
            landed(left)
            landed(right)

        @pl.when(full)
        def _():
            run([left, right], False)

        ahead(late)

    @pl.when(corner)
    def _():
        landed(me - 4 * deep + cross[2])
        run([me - 4 * deep + cross[2]], False)

    @pl.when(helped)
    def _():
        for g in range(groups):
            for copy in returns(g):
                copy.wait_recv()
            for h in range(bounds[g][0], sum(bounds[g])):
                mine = best_ref[h]
                other = back_top[h]
                top = jnp.maximum(mine, other)
                keep = jnp.exp2(mine - top)
                add = jnp.exp2(other - top)
                acc_ref[h, :VDIM] = acc_ref[h, :VDIM] * keep + back[h].astype(jnp.float32) * add
                acc_ref[h, VDIM:] = acc_ref[h, VDIM:] * keep + add

    loads[14].wait()

    def settle(at):
        flat = []
        for h in range(heads):
            acc = acc_ref[h, :, at]
            flat.append(acc[:VDIM] * (1.0 / acc[VDIM : VDIM + 1]))
        return jnp.concatenate(flat, 0).T.astype(jnp.bfloat16)

    if short % LANES:
        att[...] = settle(slice(None))

    model = cpart.shape[1]
    step = model // CHUNKS

    def rows_of(owner):
        at = pl.ds(pl.multiple_of(owner * short, short), short)
        return at, (att[at, :] if short % LANES else settle(at))

    def part(at, mixed, c):
        cols = slice(c * step, (c + 1) * step)
        return (cpart[at, cols] + dot(mixed, aproj_ref[:, cols])).astype(jnp.bfloat16)

    tails = []
    for o, mate in enumerate(mates):
        at, mixed = rows_of(mate)
        for c in range(CHUNKS):
            cols = pl.ds(c * step, step)
            part_buf[o, :, cols] = part(at, mixed, c)
            tails.append(
                pltpu.make_async_remote_copy(
                    part_buf.at[o, :, cols], in_buf.at[o, :, cols], tail_send.at[o, c], tail_recv.at[o, c],
                    device_id=(me, mate), device_id_type=MESH,
                )
            )
            tails[-1].start()
    at, mixed = rows_of(t)
    for c in range(CHUNKS):
        cpart[:short, c * step : (c + 1) * step] = part(at, mixed, c).astype(jnp.float32)
    for c in range(CHUNKS):
        cols = slice(c * step, (c + 1) * step)
        result = cpart[:short, cols]
        for o in range(len(mates)):
            tails[o * CHUNKS + c].wait_recv()
            result = result + in_buf[o, :, cols].astype(jnp.float32)
        out_ref[:, cols] = result.astype(jnp.bfloat16)
    for copy in tails + token_sends + shares(me) + query_sends:
        copy.wait_send()

    @pl.when(me + 1 < total)
    def _():
        rim_copy.wait_send()

    lift(0, finish, (1, 2, 3))
    own_side(finish, (0, 1, 2))

    @pl.when(helped)
    def _():
        ask.wait_send()

    @pl.when(helper)
    def _():
        for copy in far_shares:
            copy.wait_send()
        for g in range(groups):
            for copy in returns(g):
                copy.wait_send()

    @pl.when(jnp.logical_or(b0 == 1, helper))
    def _():
        for copy in shares(me + cross[0]):
            copy.wait_send()

    @pl.when(jnp.logical_or(b1 == 1, helper))
    def _():
        for copy in shares(me + cross[1]) + shares(me + cross[2]):
            copy.wait_send()

    @pl.loop(1, deep + 1)
    def _(d):
        j = me - 4 * d
        lift(d, finish, (1, 2, 3))
        for k in range(3):
            send(j, me + cross[k], side_send.at[d, k]).wait_send()
        for c in (0,) + cross:
            for copy in shares(j + c):
                copy.wait_send()


def local(
    tokens,
    outer_gate,
    inner_gate,
    conv_input,
    conv_taps,
    query_down,
    latent_down,
    rotary_down,
    query_gain,
    latent_gain,
    query_up,
    latent_up,
    conv_project,
    attend_project,
):
    rows = tokens.shape[0]
    heads = query_up.shape[1] // (NOPE + ROPE)
    ways = lax.axis_size("tp")
    blocks = lax.axis_size("sp")
    model = conv_project.shape[1]
    kvr = latent_up.shape[0]
    channels = conv_project.shape[0]
    half = ROPE // 2
    inverse = jnp.asarray(np.float32(rotary_base) ** (-(np.arange(half, dtype=np.float32) * 2.0 / (2 * half))), jnp.float32)
    vmem = pl.BlockSpec(memory_space=pltpu.VMEM)
    dma = pltpu.SemaphoreType.DMA
    mates = ways - 1
    ring = min(heads, RING)
    groups = 1 if heads % 4 else 2
    big = (
        inverse[:, None], tokens, latent_down, rotary_down.T, query_down, latent_up, inner_gate, conv_input,
        latent_gain[None, :], query_gain[None, :], query_up, conv_taps, outer_gate, conv_project, attend_project,
    )

    def half_type(*shape):
        return pltpu.VMEM(shape, jnp.bfloat16)

    def full_type(*shape):
        return pltpu.VMEM(shape, jnp.float32)

    return pl.pallas_call(
        mix_kernel,
        out_shape=pltpu.VMEM((rows // ways, model), jnp.bfloat16),
        in_specs=[pl.BlockSpec(memory_space=pl.ANY)] * len(big),
        out_specs=vmem,
        scratch_shapes=[pltpu.VMEM(array.shape, array.dtype) for array in big]
        + [
            half_type(mates, *tokens.shape),
            half_type(tokens.shape[1] * ways, 2 * LANES),
            half_type(ways, rows, query_down.shape[1]),
            half_type(EDGE, channels),
            half_type(EDGE, channels),
            full_type(EDGE + rows, channels),
            half_type(rows, channels),
            half_type(kvr, heads * NOPE),
            half_type(heads * VDIM, kvr),
            half_type(heads, 2 * NOPE + LANES, rows),
            half_type(blocks, ways, rows + ROPE + TAG, kvr // ways),
            half_type(2 * rows, heads * NOPE),
            half_type(heads, VDIM + ONES, 2 * rows),
            full_type(ring, 2 * rows, rows),
            half_type(ring, 2 * rows, rows),
            full_type(heads, 1, rows),
            full_type(heads, VDIM + ONES, rows),
            half_type(rows, heads * VDIM),
            full_type(rows, 2 * LANES + query_down.shape[1]),
            full_type(rows, channels),
            full_type(rows, model),
            half_type(mates, rows // ways, model),
            half_type(mates, rows // ways, model),
            half_type(ways, rows, query_down.shape[1]),
            half_type(heads, 2 * NOPE + LANES, rows),
            full_type(heads, 1, rows),
            full_type(heads, VDIM + ONES, rows),
            half_type(heads, VDIM, rows),
            full_type(heads, 1, rows),
            dma((len(big),)),
            dma((5, mates)),
            dma((5, mates)),
            dma((blocks // 4, 3)),
            dma((blocks // 4, 3)),
            dma((blocks,)),
            dma((blocks, mates)),
            dma((blocks, mates)),
            dma((mates, CHUNKS)),
            dma((mates, CHUNKS)),
            dma((2,)),
            dma((groups, 2)),
            dma((groups, 2)),
        ],
        compiler_params=pltpu.CompilerParams(
            vmem_limit_bytes=60 * 1024 * 1024, collective_id=0, has_side_effects=True
        ),
    )(*big)


def solution(mesh):
    split = P(None, "tp")
    in_specs = (P("sp", "tp"),) + (split,) * 6 + (P(),) * 3 + (split,) * 2 + (P("tp", None),) * 2
    out_specs = P(("sp", "tp"), None)
    return jax.shard_map(local, mesh=mesh, in_specs=in_specs, out_specs=out_specs, check_vma=False)
```

```python
import jax
import numpy as np
import jax.numpy as jnp
from jax import lax
from jax.experimental import pallas as pl
from jax.experimental.pallas import tpu as pltpu
from jax.sharding import PartitionSpec as P

NOPE = 64
ROPE = 32
VDIM = 64
LANES = 128
ONES = 16
EDGE = 16
RING = 8
LAG = 2
EAGER = 9
CHUNKS = 2
TAG = 16

MESH = pl.DeviceIdType.MESH
neg_fill = -1e30
rotary_base = 10000.0
norm_epsilon = 1e-06
log2e = 1.4426950408889634


def dot(a, b, dims=((1,), (0,))):
    return lax.dot_general(a, b, (dims, ((), ())), preferred_element_type=jnp.float32)


def unit(lat_parts, rot_parts, factors, qx_ref, wk_ref, wvt_ref, keys, turned, scores, weights, best_ref, acc_ref, masked, low, heads):
    latent = jnp.concatenate(lat_parts, 0)
    rot = jnp.concatenate(rot_parts, 0)
    span = latent.shape[0]
    lanes = slice(low * NOPE, (low + heads) * NOPE)
    down = jnp.concatenate([f[0] for f in factors], 0)
    along = jnp.concatenate([f[1] for f in factors], 1)
    keys[:span, lanes] = (dot(latent, wk_ref[:, lanes]) * down).astype(jnp.bfloat16)
    flat = dot(wvt_ref[low * VDIM : (low + heads) * VDIM], latent, ((1,), (1,)))
    flat = (flat * along).astype(jnp.bfloat16)
    for h in range(heads):
        turned[low + h, :VDIM, :span] = flat[h * VDIM : (h + 1) * VDIM]
    ring = scores.shape[0]
    tops = {}

    def score(h):
        pair = h // 2 * 2 * NOPE
        key = jnp.concatenate([keys[:span, pair : pair + 2 * NOPE], rot], 1)
        s = dot(key, qx_ref[h])
        if masked:
            k_at = lax.broadcasted_iota(jnp.int32, s.shape, 0)
            q_at = lax.broadcasted_iota(jnp.int32, s.shape, 1)
            s = jnp.where(k_at <= q_at, s, neg_fill)
        scores[h % ring, :span] = s
        top = jnp.max(s, 0, keepdims=True)
        if masked:
            tops[h] = (top, None)
        else:
            old = best_ref[h]
            top = jnp.maximum(old, top)
            tops[h] = (top, jnp.exp2(old - top))
        best_ref[h] = top

    def soften(h):
        weights[h % ring, :span] = jnp.exp2((scores[h % ring, :span] - tops[h][0]).astype(jnp.bfloat16))

    def gather(h):
        fresh = dot(turned[h, :, :span], weights[h % ring, :span])
        acc_ref[h] = fresh if masked else acc_ref[h] * tops[h][1] + fresh

    for step in range(heads + 2 * LAG):
        if step < heads:
            score(low + step)
        if 0 <= step - LAG < heads:
            soften(low + step - LAG)
        if 0 <= step - 2 * LAG < heads:
            gather(low + step - 2 * LAG)


def mix_kernel(
    inv_in, tok_in, ldown_in, rdown_in, qdown_in, up_in, inner_in, signal_in, lgain_in, qgain_in, qup_in, taps_in, outer_in, cproj_in, aproj_in,
    out_ref,
    inv_ref, tok, ldown, rdown, qdown, up_ref, inner_w, signal_w, lgain_ref, qgain_ref, qup, taps_ref, outer_w, cproj_ref, aproj_ref,
    xbuf, comb, raw_query, edge, rim, padded, conv_ref, wk_ref, wvt_ref, qx_ref,
    kv, keys, turned, scores, weights, best_ref, acc_ref, att, small, held, cpart, part_buf, in_buf, far_query, far_qx, far_best, far_acc, back, back_top,
    load_sem, front_send, front_recv, up_send, side_send, kv_recv, share_send, share_recv, tail_send, tail_recv, far_sem, back_send, back_recv,
):
    me = lax.axis_index("sp")
    t = lax.axis_index("tp")
    total = lax.axis_size("sp")
    ways = lax.axis_size("tp")
    planes = total // 4
    z = me // 4
    b0 = me % 2
    b1 = (me // 2) % 2
    heads, _, rows = qx_ref.shape
    short = rows // ways
    span = 4 * (planes - 1)
    helper = z == 0
    helped = z == planes - 1
    deep = lax.select(helped, z - 1, z)
    cross = (1 - 2 * b0, 2 - 4 * b1, 3 - 2 * b0 - 4 * b1)
    after = lax.rem(me + 1, total)
    before = lax.rem(me + total - 1, total)
    mates = [lax.rem(t + o, ways) for o in range(1, ways)]

    barrier = pltpu.get_barrier_semaphore()
    targets = [(me, mate) for mate in mates] + [(me + c, t) for c in cross]
    targets += [(lax.rem(me + 4 * d, total), t) for d in range(1, planes)]
    for target in targets:
        pl.semaphore_signal(barrier, inc=1, device_id=target, device_id_type=MESH)

    @pl.when(me > 0)
    def _():
        pl.semaphore_signal(barrier, inc=1, device_id=(before, t), device_id_type=MESH)

    @pl.when(me + 1 < total)
    def _():
        pl.semaphore_signal(barrier, inc=1, device_id=(after, t), device_id_type=MESH)

    ends = (me == 0).astype(jnp.int32) + (me + 1 == total).astype(jnp.int32)

    pairs = (
        (tok_in, tok), (ldown_in, ldown), (rdown_in, rdown), (qdown_in, qdown), (inv_in, inv_ref),
        (lgain_in, lgain_ref), (qgain_in, qgain_ref), (taps_in, taps_ref), (inner_in, inner_w), (up_in, up_ref),
        (qup_in, qup), (signal_in, signal_w), (outer_in, outer_w), (cproj_in, cproj_ref), (aproj_in, aproj_ref),
    )
    loads = [pltpu.make_async_copy(a, b, load_sem.at[i]) for i, (a, b) in enumerate(pairs)]
    for copy in loads[:EAGER]:
        copy.start()

    pl.semaphore_wait(barrier, len(targets) + 2 - ends)
    loads[0].wait()

    def to_mates(source, slots, kind):
        return [
            pltpu.make_async_remote_copy(
                source, slots.at[o], front_send.at[kind, o], front_recv.at[kind, o],
                device_id=(me, mate), device_id_type=MESH,
            )
            for o, mate in enumerate(mates)
        ]

    token_sends = to_mates(tok, xbuf, 0)
    for copy in token_sends:
        copy.start()
    loads[4].wait()
    half = ROPE // 2

    def turner(rank):
        position = (rank * rows + lax.broadcasted_iota(jnp.int32, (1, rows), 1)).astype(jnp.float32)
        angle = inv_ref[...] * position
        cosine = jnp.cos(angle)
        sine = jnp.sin(angle)

        def rotated(values):
            a = values[:half]
            b = values[half:]
            return jnp.concatenate([a * cosine - b * sine, a * sine + b * cosine], 0).astype(jnp.bfloat16)

        return rotated

    rotated = turner(me)
    for h in range(heads):
        turned[h, VDIM:] = jnp.ones((ONES, turned.shape[2]), jnp.bfloat16)
    depth = tok.shape[1]

    def rows_from(weight, o):
        at = pl.multiple_of(lax.rem(t + ways - o, ways) * depth, depth)
        return weight[pl.ds(at, depth), :]

    def project(x, weight, o):
        return dot(x, rows_from(weight, o))

    def rest(value, weight):
        more = project(xbuf[0], weight, 1)
        for o in range(2, ways):
            more = more + project(xbuf[o - 1], weight, o)
        return value + more

    for copy in loads[1:4]:
        copy.wait()
    for copy in loads[EAGER:]:
        copy.start()
    wide = kv.shape[3]
    if wide < LANES:
        comb[:, :LANES] = jnp.zeros((comb.shape[0], LANES), jnp.bfloat16)
    comb[:, :wide] = ldown[...]
    tall = jnp.concatenate([rdown[...].astype(jnp.float32), jnp.zeros((LANES - ROPE, comb.shape[0]), jnp.float32)], 0)
    comb[:, LANES:] = tall.T.astype(jnp.bfloat16)
    small[:, : 2 * LANES] = project(tok[...], comb, 0)
    small[:, 2 * LANES :] = project(tok[...], qdown, 0)
    for copy in token_sends:
        copy.wait_recv()
    both = rest(small[:, : 2 * LANES], comb)
    raw_query[ways - 1] = rest(small[:, 2 * LANES :], qdown).astype(jnp.bfloat16)
    piece = both[:, :wide].astype(jnp.bfloat16)
    kv[me, t, :rows] = piece
    mass = piece.astype(jnp.float32)
    mass = jnp.sum(mass * mass, -1, keepdims=True)
    lane = lax.broadcasted_iota(jnp.int32, (1, LANES), 1)
    turn = jnp.where(lane == ROPE, mass, both[:, LANES:]).T
    spun = rotated(turn[:ROPE])
    for s in range(ways):

        @pl.when(t == s)
        def _():
            kv[me, s, rows : rows + ROPE] = spun[:, s * wide : (s + 1) * wide]

    mass = turn[ROPE : ROPE + 1]
    high = mass.astype(jnp.bfloat16).astype(jnp.float32)
    folds = rows // wide
    tags = [part[:, r * wide : (r + 1) * wide] for part in (high, mass - high) for r in range(folds)]
    if len(tags) < TAG:
        tags.append(jnp.zeros((TAG - len(tags), wide), jnp.float32))
    kv[me, t, rows + ROPE :] = jnp.concatenate(tags, 0).astype(jnp.bfloat16)

    def whole(raw, gain_ref):
        values = jnp.concatenate([raw[lax.rem(t + ways - 1 - s, ways)] for s in range(ways)], 1).astype(jnp.float32)
        factor = lax.rsqrt(jnp.mean(values * values, -1, keepdims=True) + norm_epsilon)
        return (values * factor * gain_ref[...]).astype(jnp.bfloat16)

    def send(j, target, sem):
        return pltpu.make_async_remote_copy(
            kv.at[j, t], kv.at[j, t], sem, kv_recv.at[j], device_id=(target, t), device_id_type=MESH
        )

    def shares(j):
        return [
            pltpu.make_async_remote_copy(
                kv.at[j, t], kv.at[j, t], share_send.at[j, o], share_recv.at[j, o],
                device_id=(me, mate), device_id_type=MESH,
            )
            for o, mate in enumerate(mates)
        ]

    def landed(j):
        for o in range(len(mates)):
            source = lax.rem(t + ways - 1 - o, ways)
            pltpu.make_async_remote_copy(
                kv.at[j, source], kv.at[j, source], share_send.at[j, o], share_recv.at[j, o],
                device_id=(me, mates[o]), device_id_type=MESH,
            ).wait_recv()

    def arrive(j):
        send(j, me, side_send.at[0, 0]).wait_recv()

    def collect(j):
        arrive(j)
        for copy in shares(j):
            copy.start()

    def lift(d, go, steps):
        for step in steps:
            starts = d % 4 == 0 if step > 1 else jnp.logical_or(d % 4 == 0, d % 4 == 3)

            @pl.when(jnp.logical_and(starts, z + step < planes - (z == d).astype(jnp.int32)))
            def _():
                go(send(me - 4 * d, me + 4 * step, up_send.at[d // 4 * 2 + d % 4 // 3, step - 1]))

    def pass_on(d, ks):
        for k in ks:
            send(me - 4 * d, me + cross[k], side_send.at[d, k]).start()

    def relay(d, ks=(0, 1, 2)):
        j = me - 4 * d
        arrive(j)
        lift(d, begin, (1, 2, 3))
        pass_on(d, ks)
        for copy in shares(j):
            copy.start()

    def begin(copy):
        copy.start()

    def finish(copy):
        copy.wait_send()

    def own_side(go, ks):
        for k in ks:

            @pl.when(jnp.logical_or((b0, b1, b1)[k] == 0, helper))
            def _():
                go(send(me, me + cross[k], side_send.at[0, k]))

    query_sends = to_mates(raw_query.at[ways - 1], raw_query, 2)
    for copy in query_sends:
        copy.start()
    ask = pltpu.make_async_remote_copy(
        raw_query.at[ways - 1], far_query.at[ways - 1], far_sem.at[0], far_sem.at[1],
        device_id=(lax.rem(me + 4, total), t), device_id_type=MESH,
    )

    @pl.when(helped)
    def _():
        ask.start()

    lift(0, begin, (1,))
    own_side(begin, (0, 1))
    for copy in shares(me):
        copy.start()
    loads[8].wait()
    inner = rest(project(tok[...], inner_w, 0), inner_w)
    loads[11].wait()
    signal = rest(project(tok[...], signal_w, 0), signal_w)
    gated = (inner * signal).astype(jnp.bfloat16)
    padded[EDGE:] = gated.astype(jnp.float32)
    edge[...] = gated[rows - EDGE :]
    rim_copy = pltpu.make_async_remote_copy(
        edge, rim, front_send.at[3, 0], front_recv.at[3, 0], device_id=(after, t), device_id_type=MESH
    )

    @pl.when(me + 1 < total)
    def _():
        rim_copy.start()

    loads[5].wait()
    loads[9].wait()
    low = lax.broadcasted_iota(jnp.int32, (1, 2 * NOPE), 1) < NOPE
    width = NOPE + VDIM
    gain = jnp.concatenate([lgain_ref[...], jnp.zeros((LANES - 1, lgain_ref.shape[1]), jnp.float32)], 0).T[:, :1]
    for p in range(heads // 2):
        even = up_ref[:, 2 * p * width : (2 * p + 1) * width].astype(jnp.float32) * gain
        odd = up_ref[:, (2 * p + 1) * width : (2 * p + 2) * width].astype(jnp.float32) * gain
        at = slice(p * width, (p + 1) * width)
        wk_ref[:, at] = jnp.where(low, even, pltpu.roll(odd, NOPE, 1)).astype(jnp.bfloat16)
        wvt_ref[at] = jnp.where(low, pltpu.roll(even, NOPE, 1), odd).T.astype(jnp.bfloat16)

    loads[6].wait()
    loads[10].wait()
    for copy in query_sends:
        copy.wait_recv()
    def prepare(raw, spin, queries):
        scale = (NOPE + ROPE) ** (-0.5) * log2e
        query = (dot(whole(raw, qgain_ref), qup[...]) * scale).T
        size = NOPE + ROPE
        for h in range(heads):
            base = h * size
            side = h % 2 * NOPE
            queries[h, side : side + NOPE] = query[base : base + NOPE].astype(jnp.bfloat16)
            queries[h, NOPE - side : 2 * NOPE - side] = jnp.zeros((NOPE, rows), jnp.bfloat16)
            queries[h, 2 * NOPE : 2 * NOPE + ROPE] = spin(query[base + NOPE : base + size])
            queries[h, 2 * NOPE + ROPE :] = jnp.zeros((LANES - ROPE, rows), jnp.bfloat16)

    prepare(raw_query, rotated, qx_ref)

    def run(blocks, masked, queries=qx_ref, best=best_ref, acc=acc_ref, low=0, count=heads):
        lat_parts = []
        rot_parts = []
        factors = []
        for j in blocks:
            lat_parts.append(jnp.concatenate([kv[j, s, :rows] for s in range(ways)], 1))
            spin = jnp.concatenate([kv[j, s, rows : rows + ROPE] for s in range(ways)], 1).astype(jnp.float32)
            tag = kv[j, 0, rows + ROPE :].astype(jnp.float32)
            for s in range(1, ways):
                tag = tag + kv[j, s, rows + ROPE :].astype(jnp.float32)
            mass = jnp.concatenate([tag[r : r + 1] + tag[folds + r : folds + r + 1] for r in range(folds)], 1)
            along = lax.rsqrt(mass * (1.0 / (ways * wide)) + norm_epsilon)
            spin = jnp.concatenate([spin, along, jnp.zeros((LANES - ROPE - 1, rows), jnp.float32)], 0).T
            rot_parts.append(spin.astype(jnp.bfloat16))
            factors.append((spin[:, ROPE : ROPE + 1], along))
        unit(
            lat_parts, rot_parts, factors, queries, wk_ref, wvt_ref, keys, turned, scores, weights, best, acc, masked, low, count
        )

    lift(0, begin, (2,))
    own_side(begin, (2,))
    loads[12].wait()
    held[...] = rest(project(tok[...], outer_w, 0), outer_w)

    @pl.when(deep > 0)
    def _():
        relay(1, (0, 1))


    landed(me)
    run([me], True)
    lift(0, begin, (3,))

    @pl.when(deep > 0)
    def _():
        pass_on(1, (2,))


    far_shares = to_mates(far_query.at[ways - 1], far_query, 4)
    groups = back_send.shape[0]
    bounds = [(g * heads // groups, heads // groups) for g in range(groups)]

    def returns(g):
        return [
            pltpu.make_async_remote_copy(
                buf.at[pl.ds(*bounds[g])], buf.at[pl.ds(*bounds[g])], back_send.at[g, i], back_recv.at[g, i],
                device_id=(lax.rem(me + span, total), t), device_id_type=MESH,
            )
            for i, buf in enumerate((back, back_top))
        ]

    @pl.when(helper)
    def _():
        ask.wait_recv()
        for copy in far_shares:
            copy.start()
        far_best[...] = jnp.full(far_best.shape, neg_fill, jnp.float32)
        far_acc[...] = jnp.zeros(far_acc.shape, jnp.float32)
        collect(me + cross[0])
        for copy in far_shares:
            copy.wait_recv()
        prepare(far_query, turner(me + span), far_qx)
        collect(me + cross[1])
        collect(me + cross[2])
        landed(me + cross[0])
        for g in range(groups):

            @pl.loop(0, 2)
            def _(p):
                if g == 0:

                    @pl.when(p == 1)
                    def _():
                        landed(me + cross[1])
                        landed(me + cross[2])

                first = me + p * cross[1]
                then = me + (1 - p) * cross[0] + p * cross[2]
                run([first, then], False, far_qx, far_best, far_acc, *bounds[g])

            for h in range(bounds[g][0], sum(bounds[g])):
                acc = far_acc[h]
                mass = acc[VDIM : VDIM + 1]
                back[h] = (acc[:VDIM] * (1.0 / mass)).astype(jnp.bfloat16)
                back_top[h] = far_best[h] + jnp.log2(mass)
            for copy in returns(g):
                copy.start()

    lower = jnp.logical_not(helper)
    corner = jnp.logical_and(b0 == 0, deep > 0)

    @pl.when(jnp.logical_and(b0 == 1, lower))
    def _():
        collect(me + cross[0])
        landed(me + cross[0])

    alone = lax.select(corner, me - 4, me + cross[0])

    @pl.when(corner)
    def _():
        landed(alone)

    @pl.when(jnp.logical_or(b0 == 1, corner))
    def _():
        run([alone], False)

    @pl.when(jnp.logical_and(b1 == 1, lower))
    def _():
        collect(me + cross[1])
        collect(me + cross[2])

    def convolve():
        loads[7].wait()

        @pl.when(me > 0)
        def _():
            rim_copy.wait_recv()
            padded[:EDGE] = rim[...].astype(jnp.float32)

        @pl.when(me == 0)
        def _():
            padded[:EDGE] = jnp.zeros((EDGE, padded.shape[1]), jnp.float32)

        reach = taps_ref.shape[0] - 1
        taps = taps_ref[...].astype(jnp.float32)
        filtered = padded[EDGE:] * taps[reach : reach + 1, :]
        for k in range(reach):
            filtered = filtered + padded[EDGE - reach + k : EDGE - reach + k + rows] * taps[k : k + 1, :]
        conv_ref[...] = (held[...] * filtered).astype(jnp.bfloat16)

        loads[13].wait()
        cpart[...] = dot(conv_ref[...], cproj_ref[...])

    @pl.loop(0, 2 * deep + 1)
    def _(n):
        plane = (n + 1) // 2
        odd = n % 2
        own = me - 4 * plane

        def ahead(when):
            then = me - 4 * ((n + 2) // 2)

            @pl.when(jnp.logical_and(when, jnp.logical_and(n < 2 * deep, odd == 0)))
            def _():
                collect(then + cross[0])

            @pl.when(jnp.logical_and(when, jnp.logical_and(n < 2 * deep, jnp.logical_xor(odd == 1, corner))))
            def _():
                collect(then + cross[1])

            @pl.when(jnp.logical_and(when, jnp.logical_and(n < 2 * deep, odd == 1)))
            def _():
                collect(then + cross[2])

        @pl.when(jnp.logical_and(n == 0, b1 == 1))
        def _():
            convolve()

        late = jnp.logical_and(n == 1, b1 == 0)
        ahead(jnp.logical_not(late))
        far = (n + b1) // 2 + 2

        @pl.when(jnp.logical_and(jnp.logical_or(n == 0, (n + b1) % 2 == 0), far <= deep))
        def _():
            relay(far)

        @pl.when(jnp.logical_and(n == 0, b1 == 0))
        def _():
            convolve()

        turned_order = jnp.logical_and(corner, n > 0)
        left = lax.select(turned_order, own + odd * cross[0] + (1 - odd) * cross[2], own + (1 - odd) * cross[1])
        right = lax.select(
            turned_order, own + odd * cross[1] - (1 - odd) * 4, own + odd * cross[0] + (1 - odd) * cross[2]
        )
        full = jnp.logical_and(n + b1 > 0, jnp.logical_not(jnp.logical_and(corner, n == 2 * deep)))

        @pl.when(jnp.logical_and(full, lower))
        def _():
            landed(left)
            landed(right)

        @pl.when(full)
        def _():
            run([left, right], False)

        ahead(late)

    @pl.when(corner)
    def _():
        landed(me - 4 * deep + cross[2])
        run([me - 4 * deep + cross[2]], False)

    @pl.when(helped)
    def _():
        for g in range(groups):
            for copy in returns(g):
                copy.wait_recv()
            for h in range(bounds[g][0], sum(bounds[g])):
                mine = best_ref[h]
                other = back_top[h]
                top = jnp.maximum(mine, other)
                keep = jnp.exp2(mine - top)
                add = jnp.exp2(other - top)
                acc_ref[h, :VDIM] = acc_ref[h, :VDIM] * keep + back[h].astype(jnp.float32) * add
                acc_ref[h, VDIM:] = acc_ref[h, VDIM:] * keep + add

    loads[14].wait()

    def settle(at):
        flat = []
        for h in range(heads):
            acc = acc_ref[h, :, at]
            flat.append(acc[:VDIM] * (1.0 / acc[VDIM : VDIM + 1]))
        return jnp.concatenate(flat, 0).T.astype(jnp.bfloat16)

    if short % LANES:
        att[...] = settle(slice(None))

    model = cpart.shape[1]
    step = model // CHUNKS

    def rows_of(owner):
        at = pl.ds(pl.multiple_of(owner * short, short), short)
        return at, (att[at, :] if short % LANES else settle(at))

    def part(at, mixed, c):
        cols = slice(c * step, (c + 1) * step)
        return (cpart[at, cols] + dot(mixed, aproj_ref[:, cols])).astype(jnp.bfloat16)

    tails = []
    for o, mate in enumerate(mates):
        at, mixed = rows_of(mate)
        for c in range(CHUNKS):
            cols = pl.ds(c * step, step)
            part_buf[o, :, cols] = part(at, mixed, c)
            tails.append(
                pltpu.make_async_remote_copy(
                    part_buf.at[o, :, cols], in_buf.at[o, :, cols], tail_send.at[o, c], tail_recv.at[o, c],
                    device_id=(me, mate), device_id_type=MESH,
                )
            )
            tails[-1].start()
    at, mixed = rows_of(t)
    for c in range(CHUNKS):
        cpart[:short, c * step : (c + 1) * step] = part(at, mixed, c).astype(jnp.float32)
    for c in range(CHUNKS):
        cols = slice(c * step, (c + 1) * step)
        result = cpart[:short, cols]
        for o in range(len(mates)):
            tails[o * CHUNKS + c].wait_recv()
            result = result + in_buf[o, :, cols].astype(jnp.float32)
        out_ref[:, cols] = result.astype(jnp.bfloat16)
    for copy in tails + token_sends + shares(me) + query_sends:
        copy.wait_send()

    @pl.when(me + 1 < total)
    def _():
        rim_copy.wait_send()

    lift(0, finish, (1, 2, 3))
    own_side(finish, (0, 1, 2))

    @pl.when(helped)
    def _():
        ask.wait_send()

    @pl.when(helper)
    def _():
        for copy in far_shares:
            copy.wait_send()
        for g in range(groups):
            for copy in returns(g):
                copy.wait_send()

    @pl.when(jnp.logical_or(b0 == 1, helper))
    def _():
        for copy in shares(me + cross[0]):
            copy.wait_send()

    @pl.when(jnp.logical_or(b1 == 1, helper))
    def _():
        for copy in shares(me + cross[1]) + shares(me + cross[2]):
            copy.wait_send()

    @pl.loop(1, deep + 1)
    def _(d):
        j = me - 4 * d
        lift(d, finish, (1, 2, 3))
        for k in range(3):
            send(j, me + cross[k], side_send.at[d, k]).wait_send()
        for c in (0,) + cross:
            for copy in shares(j + c):
                copy.wait_send()


def local(
    tokens,
    outer_gate,
    inner_gate,
    conv_input,
    conv_taps,
    query_down,
    latent_down,
    rotary_down,
    query_gain,
    latent_gain,
    query_up,
    latent_up,
    conv_project,
    attend_project,
):
    rows = tokens.shape[0]
    heads = query_up.shape[1] // (NOPE + ROPE)
    ways = lax.axis_size("tp")
    blocks = lax.axis_size("sp")
    model = conv_project.shape[1]
    kvr = latent_up.shape[0]
    channels = conv_project.shape[0]
    half = ROPE // 2
    inverse = jnp.asarray(np.float32(rotary_base) ** (-(np.arange(half, dtype=np.float32) * 2.0 / (2 * half))), jnp.float32)
    vmem = pl.BlockSpec(memory_space=pltpu.VMEM)
    dma = pltpu.SemaphoreType.DMA
    mates = ways - 1
    ring = min(heads, RING)
    groups = 1 if heads % 4 else 2
    big = (
        inverse[:, None], tokens, latent_down, rotary_down.T, query_down, latent_up, inner_gate, conv_input,
        latent_gain[None, :], query_gain[None, :], query_up, conv_taps, outer_gate, conv_project, attend_project,
    )

    def half_type(*shape):
        return pltpu.VMEM(shape, jnp.bfloat16)

    def full_type(*shape):
        return pltpu.VMEM(shape, jnp.float32)

    return pl.pallas_call(
        mix_kernel,
        out_shape=pltpu.VMEM((rows // ways, model), jnp.bfloat16),
        in_specs=[pl.BlockSpec(memory_space=pl.ANY)] * len(big),
        out_specs=vmem,
        scratch_shapes=[pltpu.VMEM(array.shape, array.dtype) for array in big]
        + [
            half_type(mates, *tokens.shape),
            half_type(tokens.shape[1] * ways, 2 * LANES),
            half_type(ways, rows, query_down.shape[1]),
            half_type(EDGE, channels),
            half_type(EDGE, channels),
            full_type(EDGE + rows, channels),
            half_type(rows, channels),
            half_type(kvr, heads * NOPE),
            half_type(heads * VDIM, kvr),
            half_type(heads, 2 * NOPE + LANES, rows),
            half_type(blocks, ways, rows + ROPE + TAG, kvr // ways),
            half_type(2 * rows, heads * NOPE),
            half_type(heads, VDIM + ONES, 2 * rows),
            full_type(ring, 2 * rows, rows),
            half_type(ring, 2 * rows, rows),
            full_type(heads, 1, rows),
            full_type(heads, VDIM + ONES, rows),
            half_type(rows, heads * VDIM),
            full_type(rows, 2 * LANES + query_down.shape[1]),
            full_type(rows, channels),
            full_type(rows, model),
            half_type(mates, rows // ways, model),
            half_type(mates, rows // ways, model),
            half_type(ways, rows, query_down.shape[1]),
            half_type(heads, 2 * NOPE + LANES, rows),
            full_type(heads, 1, rows),
            full_type(heads, VDIM + ONES, rows),
            half_type(heads, VDIM, rows),
            full_type(heads, 1, rows),
            dma((len(big),)),
            dma((5, mates)),
            dma((5, mates)),
            dma(((blocks // 4 + 1) // 2, 3)),
            dma((blocks // 4, 3)),
            dma((blocks,)),
            dma((blocks, mates)),
            dma((blocks, mates)),
            dma((mates, CHUNKS)),
            dma((mates, CHUNKS)),
            dma((2,)),
            dma((groups, 2)),
            dma((groups, 2)),
        ],
        compiler_params=pltpu.CompilerParams(
            vmem_limit_bytes=60 * 1024 * 1024, collective_id=0, has_side_effects=True
        ),
    )(*big)


def solution(mesh):
    split = P(None, "tp")
    in_specs = (P("sp", "tp"),) + (split,) * 6 + (P(),) * 3 + (split,) * 2 + (P("tp", None),) * 2
    out_specs = P(("sp", "tp"), None)
    return jax.shard_map(local, mesh=mesh, in_specs=in_specs, out_specs=out_specs, check_vma=False)
```

```python
import jax
import numpy as np
import jax.numpy as jnp
from jax import lax
from jax.experimental import pallas as pl
from jax.experimental.pallas import tpu as pltpu
from jax.sharding import PartitionSpec as P

NOPE = 64
ROPE = 32
VDIM = 64
LANES = 128
ONES = 16
EDGE = 16
RING = 8
LAG = 2
EAGER = 15
CHUNKS = 4
TAG = 16

MESH = pl.DeviceIdType.MESH
neg_fill = -1e30
rotary_base = 10000.0
norm_epsilon = 1e-06
log2e = 1.4426950408889634


def dot(a, b, dims=((1,), (0,))):
    return lax.dot_general(a, b, (dims, ((), ())), preferred_element_type=jnp.float32)


def unit(lat_parts, rot_parts, factors, qx_ref, wk_ref, wvt_ref, keys, turned, scores, weights, best_ref, acc_ref, masked, low, heads):
    latent = jnp.concatenate(lat_parts, 0)
    rot = jnp.concatenate(rot_parts, 0)
    span = latent.shape[0]
    lanes = slice(low * NOPE, (low + heads) * NOPE)
    down = jnp.concatenate([f[0] for f in factors], 0)
    along = jnp.concatenate([f[1] for f in factors], 1)
    keys[:span, lanes] = (dot(latent, wk_ref[:, lanes]) * down).astype(jnp.bfloat16)
    flat = dot(wvt_ref[low * VDIM : (low + heads) * VDIM], latent, ((1,), (1,)))
    flat = (flat * along).astype(jnp.bfloat16)
    for h in range(heads):
        turned[low + h, :VDIM, :span] = flat[h * VDIM : (h + 1) * VDIM]
    ring = scores.shape[0]
    tops = {}

    def score(h):
        pair = h // 2 * 2 * NOPE
        key = jnp.concatenate([keys[:span, pair : pair + 2 * NOPE], rot], 1)
        s = dot(key, qx_ref[h])
        if masked:
            k_at = lax.broadcasted_iota(jnp.int32, s.shape, 0)
            q_at = lax.broadcasted_iota(jnp.int32, s.shape, 1)
            s = jnp.where(k_at <= q_at, s, neg_fill)
        scores[h % ring, :span] = s
        top = jnp.max(s, 0, keepdims=True)
        if masked:
            tops[h] = (top, None)
        else:
            old = best_ref[h]
            top = jnp.maximum(old, top)
            tops[h] = (top, jnp.exp2(old - top))
        best_ref[h] = top

    def soften(h):
        weights[h % ring, :span] = jnp.exp2((scores[h % ring, :span] - tops[h][0]).astype(jnp.bfloat16))

    def gather(h):
        fresh = dot(turned[h, :, :span], weights[h % ring, :span])
        acc_ref[h] = fresh if masked else acc_ref[h] * tops[h][1] + fresh

    for step in range(heads + 2 * LAG):
        if step < heads:
            score(low + step)
        if 0 <= step - LAG < heads:
            soften(low + step - LAG)
        if 0 <= step - 2 * LAG < heads:
            gather(low + step - 2 * LAG)


def mix_kernel(
    inv_in, tok_in, ldown_in, rdown_in, qdown_in, up_in, inner_in, signal_in, lgain_in, qgain_in, qup_in, taps_in, outer_in, cproj_in, aproj_in,
    out_ref,
    inv_ref, tok, ldown, rdown, qdown, up_ref, inner_w, signal_w, lgain_ref, qgain_ref, qup, taps_ref, outer_w, cproj_ref, aproj_ref,
    xbuf, comb, raw_query, edge, rim, padded, conv_ref, wk_ref, wvt_ref, qx_ref,
    kv, keys, turned, scores, weights, best_ref, acc_ref, att, small, held, cpart, part_buf, in_buf, far_query, far_qx, far_best, far_acc, back, back_top,
    load_sem, front_send, front_recv, up_send, side_send, kv_recv, share_send, share_recv, tail_send, tail_recv, far_sem, back_send, back_recv,
):
    me = lax.axis_index("sp")
    t = lax.axis_index("tp")
    total = lax.axis_size("sp")
    ways = lax.axis_size("tp")
    planes = total // 4
    z = me // 4
    b0 = me % 2
    b1 = (me // 2) % 2
    heads, _, rows = qx_ref.shape
    short = rows // ways
    span = 4 * (planes - 1)
    helper = z == 0
    helped = z == planes - 1
    deep = lax.select(helped, z - 1, z)
    cross = (1 - 2 * b0, 2 - 4 * b1, 3 - 2 * b0 - 4 * b1)
    after = lax.rem(me + 1, total)
    before = lax.rem(me + total - 1, total)
    mates = [lax.rem(t + o, ways) for o in range(1, ways)]

    barrier = pltpu.get_barrier_semaphore()
    targets = [(me, mate) for mate in mates] + [(me + c, t) for c in cross]
    targets += [(lax.rem(me + 4 * d, total), t) for d in range(1, planes)]
    for target in targets:
        pl.semaphore_signal(barrier, inc=1, device_id=target, device_id_type=MESH)

    @pl.when(me > 0)
    def _():
        pl.semaphore_signal(barrier, inc=1, device_id=(before, t), device_id_type=MESH)

    @pl.when(me + 1 < total)
    def _():
        pl.semaphore_signal(barrier, inc=1, device_id=(after, t), device_id_type=MESH)

    ends = (me == 0).astype(jnp.int32) + (me + 1 == total).astype(jnp.int32)

    pairs = (
        (tok_in, tok), (ldown_in, ldown), (rdown_in, rdown), (qdown_in, qdown), (inv_in, inv_ref),
        (lgain_in, lgain_ref), (qgain_in, qgain_ref), (taps_in, taps_ref), (inner_in, inner_w), (up_in, up_ref),
        (qup_in, qup), (signal_in, signal_w), (outer_in, outer_w), (cproj_in, cproj_ref), (aproj_in, aproj_ref),
    )
    loads = [pltpu.make_async_copy(a, b, load_sem.at[i]) for i, (a, b) in enumerate(pairs)]
    for copy in loads[:EAGER]:
        copy.start()

    pl.semaphore_wait(barrier, len(targets) + 2 - ends)
    loads[0].wait()

    def to_mates(source, slots, kind):
        return [
            pltpu.make_async_remote_copy(
                source, slots.at[o], front_send.at[kind, o], front_recv.at[kind, o],
                device_id=(me, mate), device_id_type=MESH,
            )
            for o, mate in enumerate(mates)
        ]

    token_sends = to_mates(tok, xbuf, 0)
    for copy in token_sends:
        copy.start()
    loads[4].wait()
    half = ROPE // 2

    def turner(rank):
        position = (rank * rows + lax.broadcasted_iota(jnp.int32, (1, rows), 1)).astype(jnp.float32)
        angle = inv_ref[...] * position
        cosine = jnp.cos(angle)
        sine = jnp.sin(angle)

        def rotated(values):
            a = values[:half]
            b = values[half:]
            return jnp.concatenate([a * cosine - b * sine, a * sine + b * cosine], 0).astype(jnp.bfloat16)

        return rotated

    rotated = turner(me)
    for h in range(heads):
        turned[h, VDIM:] = jnp.ones((ONES, turned.shape[2]), jnp.bfloat16)
    depth = tok.shape[1]

    def rows_from(weight, o):
        at = pl.multiple_of(lax.rem(t + ways - o, ways) * depth, depth)
        return weight[pl.ds(at, depth), :]

    def project(x, weight, o):
        return dot(x, rows_from(weight, o))

    def rest(value, weight):
        more = project(xbuf[0], weight, 1)
        for o in range(2, ways):
            more = more + project(xbuf[o - 1], weight, o)
        return value + more

    for copy in loads[1:4]:
        copy.wait()
    for copy in loads[EAGER:]:
        copy.start()
    wide = kv.shape[3]
    if wide < LANES:
        comb[:, :LANES] = jnp.zeros((comb.shape[0], LANES), jnp.bfloat16)
    comb[:, :wide] = ldown[...]
    tall = jnp.concatenate([rdown[...].astype(jnp.float32), jnp.zeros((LANES - ROPE, comb.shape[0]), jnp.float32)], 0)
    comb[:, LANES:] = tall.T.astype(jnp.bfloat16)
    small[:, : 2 * LANES] = project(tok[...], comb, 0)
    small[:, 2 * LANES :] = project(tok[...], qdown, 0)
    for copy in token_sends:
        copy.wait_recv()
    both = rest(small[:, : 2 * LANES], comb)
    raw_query[ways - 1] = rest(small[:, 2 * LANES :], qdown).astype(jnp.bfloat16)
    piece = both[:, :wide].astype(jnp.bfloat16)
    kv[me, t, :rows] = piece
    mass = piece.astype(jnp.float32)
    mass = jnp.sum(mass * mass, -1, keepdims=True)
    lane = lax.broadcasted_iota(jnp.int32, (1, LANES), 1)
    turn = jnp.where(lane == ROPE, mass, both[:, LANES:]).T
    spun = rotated(turn[:ROPE])
    for s in range(ways):

        @pl.when(t == s)
        def _():
            kv[me, s, rows : rows + ROPE] = spun[:, s * wide : (s + 1) * wide]

    mass = turn[ROPE : ROPE + 1]
    high = mass.astype(jnp.bfloat16).astype(jnp.float32)
    folds = rows // wide
    tags = [part[:, r * wide : (r + 1) * wide] for part in (high, mass - high) for r in range(folds)]
    if len(tags) < TAG:
        tags.append(jnp.zeros((TAG - len(tags), wide), jnp.float32))
    kv[me, t, rows + ROPE :] = jnp.concatenate(tags, 0).astype(jnp.bfloat16)

    def whole(raw, gain_ref):
        values = jnp.concatenate([raw[lax.rem(t + ways - 1 - s, ways)] for s in range(ways)], 1).astype(jnp.float32)
        factor = lax.rsqrt(jnp.mean(values * values, -1, keepdims=True) + norm_epsilon)
        return (values * factor * gain_ref[...]).astype(jnp.bfloat16)

    def send(j, target, sem):
        return pltpu.make_async_remote_copy(
            kv.at[j, t], kv.at[j, t], sem, kv_recv.at[j], device_id=(target, t), device_id_type=MESH
        )

    def shares(j):
        return [
            pltpu.make_async_remote_copy(
                kv.at[j, t], kv.at[j, t], share_send.at[j, o], share_recv.at[j, o],
                device_id=(me, mate), device_id_type=MESH,
            )
            for o, mate in enumerate(mates)
        ]

    def landed(j):
        for o in range(len(mates)):
            source = lax.rem(t + ways - 1 - o, ways)
            pltpu.make_async_remote_copy(
                kv.at[j, source], kv.at[j, source], share_send.at[j, o], share_recv.at[j, o],
                device_id=(me, mates[o]), device_id_type=MESH,
            ).wait_recv()

    def arrive(j):
        send(j, me, side_send.at[0, 0]).wait_recv()

    def collect(j):
        arrive(j)
        for copy in shares(j):
            copy.start()

    def lift(d, go, steps):
        for step in steps:
            starts = d % 4 == 0 if step > 1 else jnp.logical_or(d % 4 == 0, d % 4 == 3)

            @pl.when(jnp.logical_and(starts, z + step < planes - (z == d).astype(jnp.int32)))
            def _():
                go(send(me - 4 * d, me + 4 * step, up_send.at[d // 4 * 2 + d % 4 // 3, step - 1]))

    def pass_on(d, ks):
        for k in ks:
            send(me - 4 * d, me + cross[k], side_send.at[d, k]).start()

    def relay(d, ks=(0, 1, 2)):
        j = me - 4 * d
        arrive(j)
        lift(d, begin, (1, 2, 3))
        pass_on(d, ks)
        for copy in shares(j):
            copy.start()

    def begin(copy):
        copy.start()

    def finish(copy):
        copy.wait_send()

    def own_side(go, ks):
        for k in ks:

            @pl.when(jnp.logical_or((b0, b1, b1)[k] == 0, helper))
            def _():
                go(send(me, me + cross[k], side_send.at[0, k]))

    query_sends = to_mates(raw_query.at[ways - 1], raw_query, 2)
    for copy in query_sends:
        copy.start()
    ask = pltpu.make_async_remote_copy(
        raw_query.at[ways - 1], far_query.at[ways - 1], far_sem.at[0], far_sem.at[1],
        device_id=(lax.rem(me + 4, total), t), device_id_type=MESH,
    )

    @pl.when(helped)
    def _():
        ask.start()

    lift(0, begin, (1,))
    own_side(begin, (0, 1))
    for copy in shares(me):
        copy.start()
    loads[8].wait()
    inner = rest(project(tok[...], inner_w, 0), inner_w)
    loads[11].wait()
    signal = rest(project(tok[...], signal_w, 0), signal_w)
    gated = (inner * signal).astype(jnp.bfloat16)
    padded[EDGE:] = gated.astype(jnp.float32)
    edge[...] = gated[rows - EDGE :]
    rim_copy = pltpu.make_async_remote_copy(
        edge, rim, front_send.at[3, 0], front_recv.at[3, 0], device_id=(after, t), device_id_type=MESH
    )

    @pl.when(me + 1 < total)
    def _():
        rim_copy.start()

    loads[5].wait()
    loads[9].wait()
    low = lax.broadcasted_iota(jnp.int32, (1, 2 * NOPE), 1) < NOPE
    width = NOPE + VDIM
    gain = jnp.concatenate([lgain_ref[...], jnp.zeros((LANES - 1, lgain_ref.shape[1]), jnp.float32)], 0).T[:, :1]
    for p in range(heads // 2):
        even = up_ref[:, 2 * p * width : (2 * p + 1) * width].astype(jnp.float32) * gain
        odd = up_ref[:, (2 * p + 1) * width : (2 * p + 2) * width].astype(jnp.float32) * gain
        at = slice(p * width, (p + 1) * width)
        wk_ref[:, at] = jnp.where(low, even, pltpu.roll(odd, NOPE, 1)).astype(jnp.bfloat16)
        wvt_ref[at] = jnp.where(low, pltpu.roll(even, NOPE, 1), odd).T.astype(jnp.bfloat16)

    loads[6].wait()
    loads[10].wait()
    for copy in query_sends:
        copy.wait_recv()
    def prepare(raw, spin, queries):
        scale = (NOPE + ROPE) ** (-0.5) * log2e
        query = (dot(whole(raw, qgain_ref), qup[...]) * scale).T
        size = NOPE + ROPE
        for h in range(heads):
            base = h * size
            side = h % 2 * NOPE
            queries[h, side : side + NOPE] = query[base : base + NOPE].astype(jnp.bfloat16)
            queries[h, NOPE - side : 2 * NOPE - side] = jnp.zeros((NOPE, rows), jnp.bfloat16)
            queries[h, 2 * NOPE : 2 * NOPE + ROPE] = spin(query[base + NOPE : base + size])
            queries[h, 2 * NOPE + ROPE :] = jnp.zeros((LANES - ROPE, rows), jnp.bfloat16)

    prepare(raw_query, rotated, qx_ref)

    def run(blocks, masked, queries=qx_ref, best=best_ref, acc=acc_ref, low=0, count=heads):
        lat_parts = []
        rot_parts = []
        factors = []
        for j in blocks:
            lat_parts.append(jnp.concatenate([kv[j, s, :rows] for s in range(ways)], 1))
            spin = jnp.concatenate([kv[j, s, rows : rows + ROPE] for s in range(ways)], 1).astype(jnp.float32)
            tag = kv[j, 0, rows + ROPE :].astype(jnp.float32)
            for s in range(1, ways):
                tag = tag + kv[j, s, rows + ROPE :].astype(jnp.float32)
            mass = jnp.concatenate([tag[r : r + 1] + tag[folds + r : folds + r + 1] for r in range(folds)], 1)
            along = lax.rsqrt(mass * (1.0 / (ways * wide)) + norm_epsilon)
            spin = jnp.concatenate([spin, along, jnp.zeros((LANES - ROPE - 1, rows), jnp.float32)], 0).T
            rot_parts.append(spin.astype(jnp.bfloat16))
            factors.append((spin[:, ROPE : ROPE + 1], along))
        unit(
            lat_parts, rot_parts, factors, queries, wk_ref, wvt_ref, keys, turned, scores, weights, best, acc, masked, low, count
        )

    lift(0, begin, (2,))
    own_side(begin, (2,))
    loads[12].wait()
    held[...] = rest(project(tok[...], outer_w, 0), outer_w)

    @pl.when(deep > 0)
    def _():
        relay(1, (0, 1))


    landed(me)
    run([me], True)
    lift(0, begin, (3,))

    @pl.when(deep > 0)
    def _():
        pass_on(1, (2,))


    far_shares = to_mates(far_query.at[ways - 1], far_query, 4)
    groups = back_send.shape[0]
    bounds = [(g * heads // groups, heads // groups) for g in range(groups)]

    def returns(g):
        return [
            pltpu.make_async_remote_copy(
                buf.at[pl.ds(*bounds[g])], buf.at[pl.ds(*bounds[g])], back_send.at[g, i], back_recv.at[g, i],
                device_id=(lax.rem(me + span, total), t), device_id_type=MESH,
            )
            for i, buf in enumerate((back, back_top))
        ]

    @pl.when(helper)
    def _():
        ask.wait_recv()
        for copy in far_shares:
            copy.start()
        far_best[...] = jnp.full(far_best.shape, neg_fill, jnp.float32)
        far_acc[...] = jnp.zeros(far_acc.shape, jnp.float32)
        collect(me + cross[0])
        for copy in far_shares:
            copy.wait_recv()
        prepare(far_query, turner(me + span), far_qx)
        collect(me + cross[1])
        collect(me + cross[2])
        landed(me + cross[0])
        for g in range(groups):

            @pl.loop(0, 2)
            def _(p):
                if g == 0:

                    @pl.when(p == 1)
                    def _():
                        landed(me + cross[1])
                        landed(me + cross[2])

                first = me + p * cross[1]
                then = me + (1 - p) * cross[0] + p * cross[2]
                run([first, then], False, far_qx, far_best, far_acc, *bounds[g])

            for h in range(bounds[g][0], sum(bounds[g])):
                acc = far_acc[h]
                mass = acc[VDIM : VDIM + 1]
                back[h] = (acc[:VDIM] * (1.0 / mass)).astype(jnp.bfloat16)
                back_top[h] = far_best[h] + jnp.log2(mass)
            for copy in returns(g):
                copy.start()

    lower = jnp.logical_not(helper)
    corner = jnp.logical_and(b0 == 0, deep > 0)

    @pl.when(jnp.logical_and(b0 == 1, lower))
    def _():
        collect(me + cross[0])
        landed(me + cross[0])

    alone = lax.select(corner, me - 4, me + cross[0])

    @pl.when(corner)
    def _():
        landed(alone)

    @pl.when(jnp.logical_or(b0 == 1, corner))
    def _():
        run([alone], False)

    @pl.when(jnp.logical_and(b1 == 1, lower))
    def _():
        collect(me + cross[1])
        collect(me + cross[2])

    def convolve():
        loads[7].wait()

        @pl.when(me > 0)
        def _():
            rim_copy.wait_recv()
            padded[:EDGE] = rim[...].astype(jnp.float32)

        @pl.when(me == 0)
        def _():
            padded[:EDGE] = jnp.zeros((EDGE, padded.shape[1]), jnp.float32)

        reach = taps_ref.shape[0] - 1
        taps = taps_ref[...].astype(jnp.float32)
        filtered = padded[EDGE:] * taps[reach : reach + 1, :]
        for k in range(reach):
            filtered = filtered + padded[EDGE - reach + k : EDGE - reach + k + rows] * taps[k : k + 1, :]
        conv_ref[...] = (held[...] * filtered).astype(jnp.bfloat16)

        loads[13].wait()
        cpart[...] = dot(conv_ref[...], cproj_ref[...])

    @pl.loop(0, 2 * deep + 1)
    def _(n):
        plane = (n + 1) // 2
        odd = n % 2
        own = me - 4 * plane

        def ahead(when):
            then = me - 4 * ((n + 2) // 2)

            @pl.when(jnp.logical_and(when, jnp.logical_and(n < 2 * deep, odd == 0)))
            def _():
                collect(then + cross[0])

            @pl.when(jnp.logical_and(when, jnp.logical_and(n < 2 * deep, jnp.logical_xor(odd == 1, corner))))
            def _():
                collect(then + cross[1])

            @pl.when(jnp.logical_and(when, jnp.logical_and(n < 2 * deep, odd == 1)))
            def _():
                collect(then + cross[2])

        @pl.when(jnp.logical_and(n == 0, b1 == 1))
        def _():
            convolve()

        late = jnp.logical_and(n == 1, b1 == 0)
        ahead(jnp.logical_not(late))
        far = (n + b1) // 2 + 2

        @pl.when(jnp.logical_and(jnp.logical_or(n == 0, (n + b1) % 2 == 0), far <= deep))
        def _():
            relay(far)

        @pl.when(jnp.logical_and(n == 0, b1 == 0))
        def _():
            convolve()

        turned_order = jnp.logical_and(corner, n > 0)
        left = lax.select(turned_order, own + odd * cross[0] + (1 - odd) * cross[2], own + (1 - odd) * cross[1])
        right = lax.select(
            turned_order, own + odd * cross[1] - (1 - odd) * 4, own + odd * cross[0] + (1 - odd) * cross[2]
        )
        full = jnp.logical_and(n + b1 > 0, jnp.logical_not(jnp.logical_and(corner, n == 2 * deep)))

        @pl.when(jnp.logical_and(full, lower))
        def _():
            landed(left)
            landed(right)

        @pl.when(full)
        def _():
            run([left, right], False)

        ahead(late)

    @pl.when(corner)
    def _():
        landed(me - 4 * deep + cross[2])
        run([me - 4 * deep + cross[2]], False)

    @pl.when(helped)
    def _():
        for g in range(groups):
            for copy in returns(g):
                copy.wait_recv()
            for h in range(bounds[g][0], sum(bounds[g])):
                mine = best_ref[h]
                other = back_top[h]
                top = jnp.maximum(mine, other)
                keep = jnp.exp2(mine - top)
                add = jnp.exp2(other - top)
                acc_ref[h, :VDIM] = acc_ref[h, :VDIM] * keep + back[h].astype(jnp.float32) * add
                acc_ref[h, VDIM:] = acc_ref[h, VDIM:] * keep + add

    loads[14].wait()

    def settle(at):
        flat = []
        for h in range(heads):
            acc = acc_ref[h, :, at]
            flat.append(acc[:VDIM] * (1.0 / acc[VDIM : VDIM + 1]))
        return jnp.concatenate(flat, 0).T.astype(jnp.bfloat16)

    if short % LANES:
        att[...] = settle(slice(None))

    model = cpart.shape[1]
    step = model // CHUNKS

    def rows_of(owner):
        at = pl.ds(pl.multiple_of(owner * short, short), short)
        return at, (att[at, :] if short % LANES else settle(at))

    def part(at, mixed, c):
        cols = slice(c * step, (c + 1) * step)
        return (cpart[at, cols] + dot(mixed, aproj_ref[:, cols])).astype(jnp.bfloat16)

    tails = []
    for o, mate in enumerate(mates):
        at, mixed = rows_of(mate)
        for c in range(CHUNKS):
            cols = pl.ds(c * step, step)
            part_buf[o, :, cols] = part(at, mixed, c)
            tails.append(
                pltpu.make_async_remote_copy(
                    part_buf.at[o, :, cols], in_buf.at[o, :, cols], tail_send.at[o, c], tail_recv.at[o, c],
                    device_id=(me, mate), device_id_type=MESH,
                )
            )
            tails[-1].start()
    at, mixed = rows_of(t)
    for c in range(CHUNKS):
        cpart[:short, c * step : (c + 1) * step] = part(at, mixed, c).astype(jnp.float32)
    for c in range(CHUNKS):
        cols = slice(c * step, (c + 1) * step)
        result = cpart[:short, cols]
        for o in range(len(mates)):
            tails[o * CHUNKS + c].wait_recv()
            result = result + in_buf[o, :, cols].astype(jnp.float32)
        out_ref[:, cols] = result.astype(jnp.bfloat16)
    for copy in tails + token_sends + shares(me) + query_sends:
        copy.wait_send()

    @pl.when(me + 1 < total)
    def _():
        rim_copy.wait_send()

    lift(0, finish, (1, 2, 3))
    own_side(finish, (0, 1, 2))

    @pl.when(helped)
    def _():
        ask.wait_send()

    @pl.when(helper)
    def _():
        for copy in far_shares:
            copy.wait_send()
        for g in range(groups):
            for copy in returns(g):
                copy.wait_send()

    @pl.when(jnp.logical_or(b0 == 1, helper))
    def _():
        for copy in shares(me + cross[0]):
            copy.wait_send()

    @pl.when(jnp.logical_or(b1 == 1, helper))
    def _():
        for copy in shares(me + cross[1]) + shares(me + cross[2]):
            copy.wait_send()

    @pl.loop(1, deep + 1)
    def _(d):
        j = me - 4 * d
        lift(d, finish, (1, 2, 3))
        for k in range(3):
            send(j, me + cross[k], side_send.at[d, k]).wait_send()
        for c in (0,) + cross:
            for copy in shares(j + c):
                copy.wait_send()


def local(
    tokens,
    outer_gate,
    inner_gate,
    conv_input,
    conv_taps,
    query_down,
    latent_down,
    rotary_down,
    query_gain,
    latent_gain,
    query_up,
    latent_up,
    conv_project,
    attend_project,
):
    rows = tokens.shape[0]
    heads = query_up.shape[1] // (NOPE + ROPE)
    ways = lax.axis_size("tp")
    blocks = lax.axis_size("sp")
    model = conv_project.shape[1]
    kvr = latent_up.shape[0]
    channels = conv_project.shape[0]
    half = ROPE // 2
    inverse = jnp.asarray(np.float32(rotary_base) ** (-(np.arange(half, dtype=np.float32) * 2.0 / (2 * half))), jnp.float32)
    vmem = pl.BlockSpec(memory_space=pltpu.VMEM)
    dma = pltpu.SemaphoreType.DMA
    mates = ways - 1
    ring = min(heads, RING)
    groups = 1 if heads % 4 else 2
    big = (
        inverse[:, None], tokens, latent_down, rotary_down.T, query_down, latent_up, inner_gate, conv_input,
        latent_gain[None, :], query_gain[None, :], query_up, conv_taps, outer_gate, conv_project, attend_project,
    )

    def half_type(*shape):
        return pltpu.VMEM(shape, jnp.bfloat16)

    def full_type(*shape):
        return pltpu.VMEM(shape, jnp.float32)

    return pl.pallas_call(
        mix_kernel,
        out_shape=pltpu.VMEM((rows // ways, model), jnp.bfloat16),
        in_specs=[pl.BlockSpec(memory_space=pl.ANY)] * len(big),
        out_specs=vmem,
        scratch_shapes=[pltpu.VMEM(array.shape, array.dtype) for array in big]
        + [
            half_type(mates, *tokens.shape),
            half_type(tokens.shape[1] * ways, 2 * LANES),
            half_type(ways, rows, query_down.shape[1]),
            half_type(EDGE, channels),
            half_type(EDGE, channels),
            full_type(EDGE + rows, channels),
            half_type(rows, channels),
            half_type(kvr, heads * NOPE),
            half_type(heads * VDIM, kvr),
            half_type(heads, 2 * NOPE + LANES, rows),
            half_type(blocks, ways, rows + ROPE + TAG, kvr // ways),
            half_type(2 * rows, heads * NOPE),
            half_type(heads, VDIM + ONES, 2 * rows),
            full_type(ring, 2 * rows, rows),
            half_type(ring, 2 * rows, rows),
            full_type(heads, 1, rows),
            full_type(heads, VDIM + ONES, rows),
            half_type(rows, heads * VDIM),
            full_type(rows, 2 * LANES + query_down.shape[1]),
            full_type(rows, channels),
            full_type(rows, model),
            half_type(mates, rows // ways, model),
            half_type(mates, rows // ways, model),
            half_type(ways, rows, query_down.shape[1]),
            half_type(heads, 2 * NOPE + LANES, rows),
            full_type(heads, 1, rows),
            full_type(heads, VDIM + ONES, rows),
            half_type(heads, VDIM, rows),
            full_type(heads, 1, rows),
            dma((len(big),)),
            dma((5, mates)),
            dma((5, mates)),
            dma(((blocks // 4 + 1) // 2, 3)),
            dma((blocks // 4, 3)),
            dma((blocks,)),
            dma((blocks, mates)),
            dma((blocks, mates)),
            dma((mates, CHUNKS)),
            dma((mates, CHUNKS)),
            dma((2,)),
            dma((groups, 2)),
            dma((groups, 2)),
        ],
        compiler_params=pltpu.CompilerParams(
            vmem_limit_bytes=60 * 1024 * 1024, collective_id=0, has_side_effects=True
        ),
    )(*big)


def solution(mesh):
    split = P(None, "tp")
    in_specs = (P("sp", "tp"),) + (split,) * 6 + (P(),) * 3 + (split,) * 2 + (P("tp", None),) * 2
    out_specs = P(("sp", "tp"), None)
    return jax.shard_map(local, mesh=mesh, in_specs=in_specs, out_specs=out_specs, check_vma=False)
```
